512 devices in a mesh: grp: 2 (over y), sp: 32 (over z), tp: 8 (over x, core).
Axes of the slice: x: 4, y: 2, z: 32, core: 2. Of those that a mesh axis runs over, the one named last changes fastest.
The devices are a block of a 4x8x32 slice.
Arguments:
- query_rows: bfloat16 [24576, 2048], P(('grp', 'sp'), 'tp'), parts along dimension 0, may hold values from -6 to 6, as said below
- key_rows: bfloat16 [24576, 1024], P(('grp', 'sp'), 'tp'), parts along dimension 0, may hold values from -6 to 6, as said below
- value_rows: bfloat16 [24576, 1024], P(('grp', 'sp'), 'tp'), parts along dimension 0, may hold values from -15 to 15
- pool_input: bfloat16 [24576, 2048], P(('grp', 'sp'), 'tp'), parts along dimension 0, may hold values from -6 to 6
- log_gate_sums: float32 [24576, 16], P(('grp', 'sp'), 'tp'), parts along dimension 0, as said below
- query_gain: float32 [128], replicated, may hold values from 0.7 to 4.5, as said below
- key_gain: float32 [128], replicated, may hold values from 0.7 to 4.5, as said below
- pool_weight: bfloat16 [8, 256, 256], P('tp'), may hold values from -0.375 to 0.375
- pool_scale: float32 [2048], P('tp'), may hold values from 0.1 to 1.9
- attention_out: bfloat16 [2048, 4096], P('tp'), may hold values from -0.09375 to 0.09375
- pooling_out: bfloat16 [2048, 4096], P('tp'), may hold values from -0.09375 to 0.09375
Outputs:
- mixed_rows: bfloat16 [24576, 4096], P(('grp', 'sp', 'tp')), parts along dimension 0
The draws below stay inside these ranges and needn't reach their ends.
There are 2 independent parts, one for each index of `grp`. The reference program is written for one: setup_inputs(seed, part) draws one part's arguments, and reference() takes and returns one part's arrays. A program takes and returns all parts, laid end to end along the dimension named above; an argument that names none is the same for every part. Nothing has to cross between parts.
Inputs may be any that keep to these rules, and one draw needn't show every extreme that they name: `query_rows`: normal entries; in some rows a query head's entries may equal its key head's entries of an earlier position. `key_rows`: normal entries. `log_gate_sums`: each column never rises from one position to the next. `query_gain`: Positive. `key_gain`: Positive.
All inputs are finite; a program needn't handle non-finite values.
Results may differ from the reference program's by a relative error of at most 0.014.
The reference program's roundings to bfloat16 on the way count: a program that leaves them out, or rounds other values in their place, can miss the bound.
Values may be sent and summed in bfloat16 or wider, within the bound.
A program may use at most 64 MiB of HBM per device.

```python
import math
import jax
import jax.numpy as jnp
from jax import lax

D = 4096
HEAD = 128
QUERY_HEADS = 16
KV_HEADS = 8
POOL_GROUPS = 8
GROUP = 256
MAX_WINDOW = 16
TOK_DEV = 384
SEQUENCE_TOKENS = 12288
ATT_W = 2048
POOL_W = 2048
N_TP = 8


def key_matrix(key):
    matrix = jax.random.normal(jax.random.fold_in(key, 11), (SEQUENCE_TOKENS, KV_HEADS * HEAD), jnp.float32)
    return jnp.clip(matrix, -6.0, 6.0)


def draw_key_rows(key, part):
    return key_matrix(key).astype(jnp.bfloat16)


def draw_query_rows(key, part):
    matrix = jax.random.normal(jax.random.fold_in(key, 17), (SEQUENCE_TOKENS, QUERY_HEADS * HEAD), jnp.float32)
    return jnp.clip(matrix, -6.0, 6.0).astype(jnp.bfloat16)


def gain_draw(key, salt):
    subkey = jax.random.fold_in(key, salt)
    return jax.random.uniform(subkey, (HEAD,), jnp.float32, 0.7, 1.3)


def draw_query_gain(key, part):
    return gain_draw(key, 19)


def draw_key_gain(key, part):
    return gain_draw(key, 23)


def draw_log_gate_sums(key, part):
    ranking = jax.random.permutation(jax.random.fold_in(key, 29), QUERY_HEADS)
    lasting = ranking < QUERY_HEADS // 2
    whole_loss = jax.random.uniform(jax.random.fold_in(key, 31), (QUERY_HEADS,), jnp.float32, 0.3, 0.8)
    forget_span = jax.random.uniform(jax.random.fold_in(key, 37), (QUERY_HEADS,), jnp.float32, 30.0, 100.0)
    baseline_rate = jnp.where(lasting, whole_loss / SEQUENCE_TOKENS, 1.0 / forget_span)
    span_count = SEQUENCE_TOKENS // TOK_DEV
    span_factor = jnp.exp(jax.random.uniform(jax.random.fold_in(key, 41), (span_count, 1), jnp.float32, -0.7, 0.7))
    multiplier = jnp.repeat(span_factor, TOK_DEV, axis=0)
    jaggedness = jax.random.uniform(jax.random.fold_in(key, 43), (SEQUENCE_TOKENS, QUERY_HEADS), jnp.float32, 0.2, 1.8)
    spike_positions = jax.random.randint(jax.random.fold_in(key, 47), (3,), 0, SEQUENCE_TOKENS)
    spike_depth = jax.random.uniform(jax.random.fold_in(key, 53), (3, QUERY_HEADS), jnp.float32, 0.22, 0.69)
    spike_count = (jnp.arange(SEQUENCE_TOKENS)[:, None] == spike_positions[None, :]).astype(jnp.float32)
    spike_events = jnp.dot(spike_count, spike_depth)
    return jnp.cumsum(-(baseline_rate[None, :] * multiplier * jaggedness + spike_events), axis=0)


def level_of(stream_key, shape, split, least, largest):
    gain = 1.0
    for dim, shards_of in split:
        draws = jax.random.uniform(jax.random.fold_in(jax.random.fold_in(stream_key, 6), dim), (shards_of,), jnp.float32, least / len(split), largest / len(split))
        gain = gain * jnp.repeat(jnp.exp(draws), shape[dim] // shards_of).reshape((-1,) + (1,) * (len(shape) - 1 - dim))
    return gain


def bell_draw(stream_key, dims, spread, limit, shards=(), kind=jnp.bfloat16):
    array = jax.random.normal(stream_key, dims, jnp.float32) * spread
    if len(shards) > 0:
        array = level_of(stream_key, dims, shards, -0.22, 0.18) * array
    return jnp.clip(array, min=-limit, max=limit).astype(kind)


def setup_inputs(seed: int = 0, part: int = 0) -> dict:
    streams_of = jax.random.split(jax.random.key(seed), 12)
    part_splits = jax.random.split(jax.random.fold_in(streams_of[11], part), 12)
    return {
        "query_rows": draw_query_rows(jax.random.fold_in(jax.random.fold_in(streams_of[11], part), 71), part),
        "key_rows": draw_key_rows(jax.random.fold_in(jax.random.fold_in(streams_of[11], part), 71), part),
        "value_rows": bell_draw(part_splits[2], (SEQUENCE_TOKENS, KV_HEADS * HEAD), 2.5, 15.0, ((0, 32), (1, 8))),
        "pool_input": bell_draw(part_splits[3], (SEQUENCE_TOKENS, POOL_W), 1.0, 6.0, ((0, 32), (1, 8))),
        "log_gate_sums": draw_log_gate_sums(jax.random.fold_in(jax.random.fold_in(streams_of[11], part), 71), part),
        "query_gain": draw_query_gain(jax.random.fold_in(streams_of[11], 71), part),
        "key_gain": draw_key_gain(jax.random.fold_in(streams_of[11], 71), part),
        "pool_weight": bell_draw(streams_of[7], (POOL_GROUPS, GROUP, GROUP), GROUP ** -0.5, 0.375, ((0, 8),)),
        "pool_scale": jnp.clip(1.0 + 0.18 * jax.random.normal(streams_of[8], (POOL_W,), jnp.float32), 0.1, 1.9),
        "attention_out": bell_draw(streams_of[9], (ATT_W, D), (ATT_W + POOL_W) ** -0.5, 0.09375, ((0, 8),)),
        "pooling_out": bell_draw(streams_of[10], (POOL_W, D), (ATT_W + POOL_W) ** -0.5, 0.09375, ((0, 8),)),
    }


epsilon = 1e-06
masked = -1e+30

def head_norm(row_data, gain_vector, head_count):
    shaped = row_data.astype(jnp.float32).reshape(row_data.shape[0], head_count, -1)
    scaled = shaped * lax.rsqrt(lax.optimization_barrier(jnp.mean(shaped * shaped, axis=-1, keepdims=True)) + epsilon)
    return (scaled * gain_vector).astype(jnp.bfloat16)

def window_means(padded, length, first_pos, windows):
    rim_rows = padded.shape[0] - length
    window_sum = jnp.zeros((length,) + padded.shape[1:], jnp.float32)
    pooled = window_sum
    for lookback in range(rim_rows + 1):
        window_sum = window_sum + padded[rim_rows - lookback:rim_rows - lookback + length]
        window_size = lookback + 1
        if window_size >= 2 and window_size & window_size - 1 == 0:
            pooled = jnp.where((windows == window_size)[None, :, None], window_sum, pooled)
    positions = (first_pos + jnp.arange(length, dtype=jnp.int32)).astype(jnp.float32)
    counts = jnp.minimum(positions[:, None, None] + 1.0, windows.astype(jnp.float32)[None, :, None])
    return pooled / counts - padded[rim_rows:]

def reference(query_rows, key_rows, value_rows, pool_input, log_gate_sums, query_gain, key_gain, pool_weight, pool_scale, attention_out, pooling_out):
    ratio = QUERY_HEADS // KV_HEADS
    queries = head_norm(query_rows, query_gain, QUERY_HEADS).transpose(1, 0, 2)
    normed_keys = jnp.repeat(head_norm(key_rows, key_gain, KV_HEADS), ratio, axis=1).transpose(1, 0, 2)
    values = jnp.repeat(value_rows.reshape(SEQUENCE_TOKENS, KV_HEADS, HEAD), ratio, axis=1).transpose(1, 0, 2)
    gates = log_gate_sums.T
    block_rows = math.gcd(SEQUENCE_TOKENS, 512)
    key_pos = jnp.arange(SEQUENCE_TOKENS, dtype=jnp.int32)

    def attend_head(operands):
        head_query, head_key, head_value, head_gate = operands

        def one_block(block_index):
            first = block_index * block_rows
            block_query = lax.dynamic_slice_in_dim(head_query, first, block_rows, 0)
            block_gate = lax.dynamic_slice_in_dim(head_gate, first, block_rows, 0)
            scores = jnp.dot(block_query, head_key.T, preferred_element_type=jnp.float32)
            scores = scores * (1.0 / math.sqrt(HEAD)) + block_gate[:, None] - head_gate[None, :]
            allowed = key_pos[None, :] <= (first + jnp.arange(block_rows, dtype=jnp.int32))[:, None]
            scores = jnp.where(allowed, scores, masked)
            row_best = lax.optimization_barrier(jnp.max(scores, axis=-1, keepdims=True))
            weights = jnp.where(allowed, jnp.exp(scores - row_best), 0.0)
            weight_sum = lax.optimization_barrier(jnp.sum(weights, axis=-1, keepdims=True))
            summed = jnp.dot(weights.astype(jnp.bfloat16), head_value, preferred_element_type=jnp.float32)
            return (summed / weight_sum).astype(jnp.bfloat16)
        return lax.map(one_block, jnp.arange(SEQUENCE_TOKENS // block_rows, dtype=jnp.int32)).reshape(SEQUENCE_TOKENS, HEAD)
    attended = lax.map(attend_head, (queries, normed_keys, values, gates))
    attended = attended.transpose(1, 0, 2).reshape(SEQUENCE_TOKENS, QUERY_HEADS * HEAD)
    padded = jnp.concatenate([jnp.zeros((MAX_WINDOW - 1, POOL_GROUPS * GROUP), jnp.float32), pool_input.astype(jnp.float32)])
    padded = padded.reshape(SEQUENCE_TOKENS + MAX_WINDOW - 1, POOL_GROUPS, GROUP)
    levels = MAX_WINDOW.bit_length() - 1
    windows = 2 ** (1 + jnp.arange(POOL_GROUPS, dtype=jnp.int32) % levels)
    pooled = window_means(padded, SEQUENCE_TOKENS, 0, windows).astype(jnp.bfloat16)
    mixing = jnp.einsum('tgc,gcd->tgd', pooled.astype(jnp.float32), pool_weight.astype(jnp.float32))
    pool_mixed = (mixing * pool_scale.reshape(POOL_GROUPS, GROUP)).astype(jnp.bfloat16).reshape(SEQUENCE_TOKENS, POOL_GROUPS * GROUP)
    attend_share = QUERY_HEADS * HEAD // N_TP
    pool_share = POOL_GROUPS * GROUP // N_TP
    merged = jnp.zeros((SEQUENCE_TOKENS, D), jnp.float32)
    for device in range(N_TP):
        attend_cols = attended[:, device * attend_share:(device + 1) * attend_share]
        pool_cols = pool_mixed[:, device * pool_share:(device + 1) * pool_share]
        partial_sum = jnp.dot(attend_cols, attention_out[device * attend_share:(device + 1) * attend_share], preferred_element_type=jnp.float32)
        partial_sum = partial_sum + jnp.dot(pool_cols, pooling_out[device * pool_share:(device + 1) * pool_share], preferred_element_type=jnp.float32)
        rounded = lax.optimization_barrier(partial_sum.astype(jnp.bfloat16))
        merged = merged + rounded.astype(jnp.float32)
    return merged.astype(jnp.bfloat16)
```

```python
import functools
import math

import jax
import jax.numpy as jnp
from jax import lax
from jax.experimental import pallas as pl
from jax.experimental.pallas import tpu as pltpu
from jax.sharding import PartitionSpec as P

HEAD = 128
MAX_WINDOW = 16
LANES = 128
CHUNKS = 4

epsilon = 1e-06
masked = -1e30
LOG2E = math.log2(math.e)

f32 = jnp.float32
bf16 = jnp.bfloat16


def normed(rows, gain):
    wide = rows.astype(f32)
    scale = lax.rsqrt(jnp.mean(wide * wide, axis=-1, keepdims=True) + epsilon)
    return (wide * scale * gain).astype(bf16)


def rows_dot(a, b):
    return lax.dot_general(a, b, (((1,), (1,)), ((), ())), preferred_element_type=f32)


def dot(a, b):
    return jnp.dot(a, b, preferred_element_type=f32)


def kernel(
    n_sp,
    n_tp,
    q_ref,
    k_ref,
    v_ref,
    gate_ref,
    pool_ref,
    q_gain_ref,
    k_gain_ref,
    pool_w_ref,
    pool_s_ref,
    att_w_hbm,
    pool_w_out_hbm,
    out_ref,
    keys,
    values,
    gates,
    queries,
    best,
    total,
    acc,
    mix,
    rim,
    w_att,
    w_pool,
    pool_part,
    parts,
    relay,
    landed,
    up_send,
    up_recv,
    down_send,
    down_recv,
    early_send,
    early_recv,
    local_sem,
    mix_send,
    mix_recv,
    relay_send,
    relay_recv,
    land_send,
    land_recv,
):
    me = lax.axis_index("sp")
    tp = lax.axis_index("tp")
    length = q_ref.shape[0]
    heads = q_ref.shape[1] // HEAD
    pieces = length // LANES
    n_x = n_tp // 2
    core = lax.rem(tp, 2)
    other = 1 - core
    chip = tp // 2
    chip_right = lax.rem(chip + 1, n_x)
    chip_left = lax.rem(chip + n_x - 1, n_x)
    chip_far = lax.rem(chip + 2, n_x)
    above = lax.rem(me + 1, n_sp)
    below = lax.rem(me + n_sp - 1, n_sp)
    n_up = n_sp // 2
    n_down = n_sp - 1 - n_up
    half = out_ref.shape[1] // 2
    cols = half // CHUNKS
    rows = out_ref.shape[0]

    def remote(src, dst, send_sem, recv_sem, **where):
        return pltpu.make_async_remote_copy(
            src_ref=src,
            dst_ref=dst,
            send_sem=send_sem,
            recv_sem=recv_sem,
            device_id=where,
            device_id_type=pl.DeviceIdType.MESH,
        )

    barrier = pltpu.get_barrier_semaphore()
    for where in (
        {"sp": above},
        {"sp": below},
        {"tp": 2 * chip + other},
        {"tp": 2 * chip_right},
        {"tp": 2 * chip_right + 1},
        {"tp": 2 * chip_left},
        {"tp": 2 * chip_left + 1},
    ):
        pl.semaphore_signal(
            barrier, inc=1, device_id=where, device_id_type=pl.DeviceIdType.MESH
        )

    my_cols = pl.ds(pl.multiple_of(core * half, LANES), half)
    other_cols = pl.ds(pl.multiple_of(other * half, LANES), half)
    load_att = pltpu.make_async_copy(att_w_hbm.at[:, my_cols], w_att.at[0], local_sem.at[0])
    load_pool = pltpu.make_async_copy(
        pool_w_out_hbm.at[:, my_cols], w_pool.at[0], local_sem.at[1]
    )
    load_att.start()
    load_pool.start()

    keys[me] = normed(k_ref[...], k_gain_ref[...])
    values[me] = v_ref[...]
    gates[me] = gate_ref[...]

    pl.semaphore_wait(barrier, 7)

    def ring_copies(slot, step, src_first):
        sources = (
            (v_ref, gate_ref, keys.at[slot])
            if src_first
            else (values.at[slot], gates.at[slot], keys.at[slot])
        )
        targets = (values.at[slot], gates.at[slot], keys.at[slot])
        return sources, targets

    def up_copy(kind, slot, step, src_first=False):
        sources, targets = ring_copies(slot, step, src_first)
        return remote(
            sources[kind],
            targets[kind],
            up_send.at[kind, step],
            up_recv.at[kind, step],
            sp=above,
        )

    def down_copy(kind, slot, step, src_first=False):
        sources, targets = ring_copies(slot, step, src_first)
        return remote(
            sources[kind],
            targets[kind],
            down_send.at[kind, step],
            down_recv.at[kind, step],
            sp=below,
        )

    for kind in (0, 1):
        up_copy(kind, me, 0, True).start()
        if n_down > 0:
            down_copy(kind, me, 0, True).start()
    for h in range(heads):
        queries[h] = normed(q_ref[:, h * HEAD : (h + 1) * HEAD], q_gain_ref[...])
    up_copy(2, me, 0, True).start()
    if n_down > 0:
        down_copy(2, me, 0, True).start()

    rim_copy = remote(
        pool_ref.at[pl.ds(length - MAX_WINDOW, MAX_WINDOW)],
        rim,
        early_send.at[0],
        early_recv.at[0],
        sp=above,
    )
    att_w_copy = remote(
        att_w_hbm.at[:, other_cols],
        w_att.at[1],
        early_send.at[1],
        early_recv.at[1],
        tp=2 * chip + other,
    )
    pool_w_copy = remote(
        pool_w_out_hbm.at[:, other_cols],
        w_pool.at[1],
        early_send.at[2],
        early_recv.at[2],
        tp=2 * chip + other,
    )
    rim_copy.start()
    att_w_copy.start()
    pool_w_copy.start()

    scale = LOG2E / math.sqrt(HEAD)

    def score_pieces(h, slot):
        z = rows_dot(queries[h], keys[slot])
        base = gate_ref[h * pieces : h * pieces + 1, 0:1]
        lifted = (base - gates[slot]) * LOG2E
        return [
            z[:, c * LANES : (c + 1) * LANES] * scale
            + lifted[h * pieces + c : h * pieces + c + 1, :]
            for c in range(pieces)
        ]

    def row_max(score):
        most = functools.reduce(jnp.maximum, score)
        return jnp.max(most, axis=-1, keepdims=True)

    def weigh(score, top):
        weights = [jnp.exp2(s - top) for s in score]
        return functools.reduce(jnp.add, weights), jnp.concatenate(
            [w.astype(bf16) for w in weights], axis=1
        )

    def attend_own():
        for h in range(heads):
            score = score_pieces(h, me)
            position = lax.broadcasted_iota(jnp.int32, (length, LANES), 0)
            lane = lax.broadcasted_iota(jnp.int32, (length, LANES), 1)
            score = [
                jnp.where(lane + c * LANES <= position, s, masked) for c, s in enumerate(score)
            ]
            top = jnp.broadcast_to(row_max(score), (length, LANES))
            summed, weights = weigh(score, top)
            best[h] = top
            total[h] = summed
            acc[h] = dot(weights, values[me])

    def attend(slot):
        for h in range(heads):
            score = score_pieces(h, slot)
            before = best[h]
            top = jnp.maximum(before, row_max(score))
            fade = jnp.exp2(before - top)
            summed, weights = weigh(score, top)
            best[h] = top
            total[h] = total[h] * fade + summed
            acc[h] = acc[h] * fade + dot(weights, values[slot])

    attend_own()

    level_count = MAX_WINDOW.bit_length() - 1
    level = lax.rem(tp, level_count)

    def pooling():
        rim_copy.wait_recv()
        edge = jnp.where(me > 0, rim[...].astype(f32), 0.0)
        here = pool_ref[...].astype(f32)
        window_sum = jnp.concatenate([edge, here], axis=0)
        chosen = jnp.zeros_like(here)
        for k in range(level_count):
            window_sum = window_sum + pltpu.roll(window_sum, 1 << k, 0)
            chosen = jnp.where(level == k, window_sum[MAX_WINDOW:], chosen)
        window = (2 << level).astype(f32) if hasattr(level, "astype") else float(2 << level)
        position = me * length + lax.broadcasted_iota(jnp.int32, here.shape, 0)
        counts = jnp.minimum(position.astype(f32) + 1.0, window)
        pooled = (chosen / counts - here).astype(bf16)
        mixed = dot(pooled, pool_w_ref[0]) * pool_s_ref[...]
        mix[0] = mixed.astype(bf16)

    pooling()
    partner = 2 * chip + other
    pool_mix_copy = remote(
        mix.at[0], mix.at[1], mix_send.at[0], mix_recv.at[0], tp=partner
    )

    def ring_step(step, carry):
        slot_up = lax.rem(me - step + n_sp, n_sp)
        slot_down = lax.rem(me + step, n_sp)
        for kind in range(3):
            up_copy(kind, slot_up, step - 1).wait_recv()

            @pl.when(step < n_up)
            def _():
                up_copy(kind, slot_up, step).start()

            if n_down > 0:

                @pl.when(step <= n_down)
                def _():
                    down_copy(kind, slot_down, step - 1).wait_recv()

                @pl.when(step < n_down)
                def _():
                    down_copy(kind, slot_down, step).start()

        @pl.when(step <= me)
        def _():
            attend(slot_up)

        @pl.when(jnp.logical_and(step <= n_down, me + step >= n_sp))
        def _():
            attend(slot_down)

        return carry

    lax.fori_loop(1, 2, ring_step, 0)

    pool_mix_copy.start()
    load_att.wait()
    load_pool.wait()
    att_w_copy.wait_recv()
    pool_w_copy.wait_recv()
    pool_mix_copy.wait_recv()
    for c in range(CHUNKS):
        span = pl.ds(c * cols, cols)
        pool_part[:, span] = dot(mix[0], w_pool[0, :, span]) + dot(mix[1], w_pool[1, :, span])

    lax.fori_loop(2, n_up + 1, ring_step, 0)

    for h in range(heads):
        weight_sum = jnp.sum(total[h], axis=-1, keepdims=True)
        mix[2, :, h * HEAD : (h + 1) * HEAD] = (acc[h] / weight_sum).astype(bf16)
    att_mix_copy = remote(mix.at[2], mix.at[3], mix_send.at[1], mix_recv.at[1], tp=partner)
    att_mix_copy.start()
    att_mix_copy.wait_recv()

    def relay_copies(c):
        return (
            remote(
                parts.at[2 * chip_far, c],
                relay.at[0, c],
                relay_send.at[0, c],
                relay_recv.at[0, c],
                tp=2 * chip_right + core,
            ),
            remote(
                parts.at[2 * chip_far + 1, c],
                relay.at[1, c],
                relay_send.at[1, c],
                relay_recv.at[1, c],
                tp=2 * chip_left + core,
            ),
        )

    def land_copy(side, target_chip, target_core, c):
        target = 2 * target_chip + target_core
        return remote(
            parts.at[target, c],
            landed.at[side, core, c],
            land_send.at[side, target_core, c],
            land_recv.at[side, core, c],
            tp=target,
        )

    def home_copy(c):
        return remote(
            parts.at[partner, c],
            landed.at[2, core, c],
            land_send.at[2, 0, c],
            land_recv.at[2, core, c],
            tp=partner,
        )

    for c in range(CHUNKS):
        span = pl.ds(c * cols, cols)
        part = (
            dot(mix[2], w_att[0, :, span])
            + dot(mix[3], w_att[1, :, span])
            + pool_part[:, span]
        ).astype(bf16)
        for d in range(n_tp):
            parts[d, c] = part[d * rows : (d + 1) * rows]
        for copy in relay_copies(c):
            copy.start()
    for c in range(CHUNKS):
        land_copy(0, chip_right, 1, c).start()
        land_copy(1, chip_left, 0, c).start()
    for c in range(CHUNKS):
        home_copy(c).start()
    for c in range(CHUNKS):
        from_left, from_right = relay_copies(c)
        for side, copy, target in (
            (0, from_left, 2 * chip_right),
            (1, from_right, 2 * chip_left + 1),
        ):
            copy.wait_recv()
            joined = parts[target, c].astype(f32) + relay[side, c].astype(f32)
            parts[target, c] = joined.astype(bf16)
        land_copy(0, chip_right, 0, c).start()
        land_copy(1, chip_left, 1, c).start()

    def landed_wait(side, source_core, c):
        remote(
            landed.at[side, source_core, c],
            landed.at[side, source_core, c],
            land_send.at[side, 0, c],
            land_recv.at[side, source_core, c],
            tp=partner,
        ).wait_recv()

    for c in range(CHUNKS):
        landed_wait(2, other, c)
        for source_core in range(2):
            landed_wait(0, source_core, c)
            landed_wait(1, source_core, c)
        for source_core in range(2):
            home = jnp.where(
                core == source_core,
                parts[tp, c].astype(f32),
                landed[2, source_core, c].astype(f32),
            )
            merged = (
                home
                + landed[0, source_core, c].astype(f32)
                + landed[1, source_core, c].astype(f32)
            )
            first = source_core * half + c * cols
            out_ref[:, first : first + cols] = merged.astype(bf16)

    def sent(step, carry):
        for kind in range(3):
            up_copy(kind, me, step).wait_send()
            if n_down > 0:

                @pl.when(step < n_down)
                def _():
                    down_copy(kind, me, step).wait_send()

        return carry

    lax.fori_loop(0, n_up, sent, 0)
    rim_copy.wait_send()
    att_w_copy.wait_send()
    pool_w_copy.wait_send()
    pool_mix_copy.wait_send()
    att_mix_copy.wait_send()
    for c in range(CHUNKS):
        for copy in relay_copies(c):
            copy.wait_send()
        land_copy(0, chip_right, 1, c).wait_send()
        land_copy(1, chip_left, 0, c).wait_send()
        land_copy(0, chip_right, 0, c).wait_send()
        land_copy(1, chip_left, 1, c).wait_send()
        home_copy(c).wait_send()


def body(
    n_sp,
    n_tp,
    query_rows,
    key_rows,
    value_rows,
    pool_input,
    log_gate_sums,
    query_gain,
    key_gain,
    pool_weight,
    pool_scale,
    attention_out,
    pooling_out,
):
    length = query_rows.shape[0]
    heads = query_rows.shape[1] // HEAD
    group = pool_input.shape[1]
    width = attention_out.shape[1]
    half = width // 2
    cols = half // CHUNKS
    rows = length // n_tp
    gate_rows = log_gate_sums.T.reshape(-1, LANES)
    gate_rows = jnp.pad(gate_rows, ((0, -gate_rows.shape[0] % 8), (0, 0)))
    n_up = n_sp // 2
    n_down = max(n_sp - 1 - n_up, 1)
    vmem = pl.BlockSpec(memory_space=pltpu.VMEM)
    dma = pltpu.SemaphoreType.DMA
    return pl.pallas_call(
        functools.partial(kernel, n_sp, n_tp),
        out_shape=jax.ShapeDtypeStruct((rows, width), bf16),
        in_specs=[vmem] * 9 + [pl.BlockSpec(memory_space=pl.ANY)] * 2,
        out_specs=vmem,
        scratch_shapes=[
            pltpu.VMEM((n_sp, length, HEAD), bf16),
            pltpu.VMEM((n_sp, length, HEAD), bf16),
            pltpu.VMEM((n_sp,) + gate_rows.shape, f32),
            pltpu.VMEM((heads, length, HEAD), bf16),
            pltpu.VMEM((heads, length, LANES), f32),
            pltpu.VMEM((heads, length, LANES), f32),
            pltpu.VMEM((heads, length, HEAD), f32),
            pltpu.VMEM((4, length, group), bf16),
            pltpu.VMEM((MAX_WINDOW, group), bf16),
            pltpu.VMEM((2, heads * HEAD, half), bf16),
            pltpu.VMEM((2, group, half), bf16),
            pltpu.VMEM((length, half), f32),
            pltpu.VMEM((n_tp, CHUNKS, rows, cols), bf16),
            pltpu.VMEM((2, CHUNKS, rows, cols), bf16),
            pltpu.VMEM((3, 2, CHUNKS, rows, cols), bf16),
            dma((3, n_up)),
            dma((3, n_up)),
            dma((3, n_down)),
            dma((3, n_down)),
            dma((3,)),
            dma((3,)),
            dma((2,)),
            dma((2,)),
            dma((2,)),
            dma((2, CHUNKS)),
            dma((2, CHUNKS)),
            dma((3, 2, CHUNKS)),
            dma((3, 2, CHUNKS)),
        ],
        compiler_params=pltpu.CompilerParams(
            collective_id=0, has_side_effects=True, vmem_limit_bytes=56 * 1024 * 1024
        ),
    )(
        query_rows,
        key_rows,
        value_rows,
        gate_rows,
        pool_input,
        query_gain.reshape(1, -1),
        key_gain.reshape(1, -1),
        pool_weight,
        pool_scale.reshape(1, -1),
        attention_out,
        pooling_out,
    )


def solution(mesh):
    return jax.shard_map(
        functools.partial(body, mesh.shape["sp"], mesh.shape["tp"]),
        mesh=mesh,
        in_specs=(
            P(("grp", "sp"), "tp"),
            P(("grp", "sp"), "tp"),
            P(("grp", "sp"), "tp"),
            P(("grp", "sp"), "tp"),
            P(("grp", "sp"), "tp"),
            P(),
            P(),
            P("tp", None, None),
            P("tp"),
            P("tp", None),
            P("tp", None),
        ),
        out_specs=P(("grp", "sp", "tp"), None),
        check_vma=False,
    )
```

```python
import functools
import math

import jax
import jax.numpy as jnp
from jax import lax
from jax.experimental import pallas as pl
from jax.experimental.pallas import tpu as pltpu
from jax.sharding import PartitionSpec as P

HEAD = 128
MAX_WINDOW = 16
LANES = 128
CHUNKS = 4
WRAPPED = 13
LAG = 3

epsilon = 1e-06
masked = -1e30
LOG2E = math.log2(math.e)

f32 = jnp.float32
bf16 = jnp.bfloat16


def normed(rows, gain):
    wide = rows.astype(f32)
    scale = lax.rsqrt(jnp.mean(wide * wide, axis=-1, keepdims=True) + epsilon)
    return (wide * scale * gain).astype(bf16)


def rows_dot(a, b):
    return lax.dot_general(a, b, (((1,), (1,)), ((), ())), preferred_element_type=f32)


def dot(a, b):
    return jnp.dot(a, b, preferred_element_type=f32)


def kernel(
    n_sp,
    n_tp,
    q_ref,
    k_ref,
    v_ref,
    gate_ref,
    pool_ref,
    q_gain_ref,
    k_gain_ref,
    pool_w_ref,
    pool_s_ref,
    att_w_hbm,
    pool_w_out_hbm,
    out_ref,
    keys,
    values,
    gates,
    queries,
    best,
    total,
    acc,
    mix,
    rim,
    w_att,
    w_pool,
    pool_part,
    parts,
    relay,
    landed,
    up_send,
    up_recv,
    down_send,
    down_recv,
    ready_sem,
    early_send,
    early_recv,
    local_sem,
    mix_send,
    mix_recv,
    relay_send,
    relay_recv,
    land_send,
    land_recv,
):
    me = lax.axis_index("sp")
    tp = lax.axis_index("tp")
    length = q_ref.shape[0]
    heads = q_ref.shape[1] // HEAD
    pieces = length // LANES
    n_x = n_tp // 2
    core = lax.rem(tp, 2)
    other = 1 - core
    chip = tp // 2
    chip_right = lax.rem(chip + 1, n_x)
    chip_left = lax.rem(chip + n_x - 1, n_x)
    chip_far = lax.rem(chip + 2, n_x)
    above = lax.rem(me + 1, n_sp)
    below = lax.rem(me + n_sp - 1, n_sp)
    wrapped = min(WRAPPED, (n_sp - 1) // 2)
    hops = n_sp - 1 - wrapped
    last = n_sp - 1
    half = out_ref.shape[1] // 2
    cols = half // CHUNKS
    rows = out_ref.shape[0]

    def remote(src, dst, send_sem, recv_sem, **where):
        return pltpu.make_async_remote_copy(
            src_ref=src,
            dst_ref=dst,
            send_sem=send_sem,
            recv_sem=recv_sem,
            device_id=where,
            device_id_type=pl.DeviceIdType.MESH,
        )

    barrier = pltpu.get_barrier_semaphore()
    @pl.when(me < last)
    def _():
        pl.semaphore_signal(
            barrier, inc=1, device_id={"sp": above}, device_id_type=pl.DeviceIdType.MESH
        )

    for where in (
        {"sp": below},
        {"tp": 2 * chip + other},
        {"tp": 2 * chip_right},
        {"tp": 2 * chip_right + 1},
        {"tp": 2 * chip_left},
        {"tp": 2 * chip_left + 1},
    ):
        pl.semaphore_signal(
            barrier, inc=1, device_id=where, device_id_type=pl.DeviceIdType.MESH
        )

    my_cols = pl.ds(pl.multiple_of(core * half, LANES), half)
    other_cols = pl.ds(pl.multiple_of(other * half, LANES), half)
    load_att = pltpu.make_async_copy(att_w_hbm.at[:, my_cols], w_att.at[0], local_sem.at[0])
    load_pool = pltpu.make_async_copy(
        pool_w_out_hbm.at[:, my_cols], w_pool.at[0], local_sem.at[1]
    )
    load_att.start()
    load_pool.start()

    keys[me] = normed(k_ref[...], k_gain_ref[...])
    values[me] = v_ref[...]
    gates[me] = gate_ref[...]
    for h in range(heads):
        queries[h] = normed(q_ref[:, h * HEAD : (h + 1) * HEAD], q_gain_ref[...])

    @pl.when(me == 0)
    def _():
        pl.semaphore_wait(barrier, 6)

    @pl.when(me > 0)
    def _():
        pl.semaphore_wait(barrier, 7)

    @pl.when(me == last)
    def _():
        pl.semaphore_signal(
            ready_sem, inc=1, device_id={"sp": above}, device_id_type=pl.DeviceIdType.MESH
        )

    stores = (values, gates, keys)

    def up_copy(kind, slot, step):
        return remote(
            stores[kind].at[slot],
            stores[kind].at[slot],
            up_send.at[kind, step],
            up_recv.at[kind, step],
            sp=above,
        )

    def down_copy(kind, slot):
        return remote(
            stores[kind].at[slot],
            stores[kind].at[slot],
            down_send.at[kind, slot],
            down_recv.at[kind, slot],
            sp=below,
        )

    @pl.when(me < last)
    def _():
        for kind in range(3):
            up_copy(kind, me, 0).start()

    @pl.when(jnp.logical_and(me > 0, me < wrapped))
    def _():
        for kind in range(3):
            down_copy(kind, me).start()

    rim_copy = remote(
        pool_ref.at[pl.ds(length - MAX_WINDOW, MAX_WINDOW)],
        rim,
        early_send.at[0],
        early_recv.at[0],
        sp=above,
    )
    att_w_copy = remote(
        att_w_hbm.at[:, other_cols],
        w_att.at[1],
        early_send.at[1],
        early_recv.at[1],
        tp=2 * chip + other,
    )
    pool_w_copy = remote(
        pool_w_out_hbm.at[:, other_cols],
        w_pool.at[1],
        early_send.at[2],
        early_recv.at[2],
        tp=2 * chip + other,
    )

    @pl.when(me < last)
    def _():
        rim_copy.start()

    att_w_copy.start()
    pool_w_copy.start()

    scale = LOG2E / math.sqrt(HEAD)

    def score_pieces(h, slot):
        z = rows_dot(queries[h], keys[slot])
        base = gate_ref[h * pieces : h * pieces + 1, 0:1]
        lifted = (base - gates[slot]) * LOG2E
        return [
            z[:, c * LANES : (c + 1) * LANES] * scale
            + lifted[h * pieces + c : h * pieces + c + 1, :]
            for c in range(pieces)
        ]

    def row_max(score):
        most = functools.reduce(jnp.maximum, score)
        return jnp.max(most, axis=-1, keepdims=True)

    def weigh(score, top):
        weights = [jnp.exp2(s - top) for s in score]
        return functools.reduce(jnp.add, weights), jnp.concatenate(
            [w.astype(bf16) for w in weights], axis=1
        )

    def attend_own():
        for h in range(heads):
            score = score_pieces(h, me)
            position = lax.broadcasted_iota(jnp.int32, (length, LANES), 0)
            lane = lax.broadcasted_iota(jnp.int32, (length, LANES), 1)
            score = [
                jnp.where(lane + c * LANES <= position, s, masked) for c, s in enumerate(score)
            ]
            top = jnp.broadcast_to(row_max(score), (length, LANES))
            summed, weights = weigh(score, top)
            best[h] = top
            total[h] = summed
            acc[h] = dot(weights, values[me])

    def attend(slot):
        for h in range(heads):
            score = score_pieces(h, slot)
            before = best[h]
            top = jnp.maximum(before, row_max(score))
            fade = jnp.exp2(before - top)
            summed, weights = weigh(score, top)
            best[h] = top
            total[h] = total[h] * fade + summed
            acc[h] = acc[h] * fade + dot(weights, values[slot])

    attend_own()

    level_count = MAX_WINDOW.bit_length() - 1
    level = lax.rem(tp, level_count)

    def pooling():
        @pl.when(me == 0)
        def _():
            rim[...] = jnp.zeros_like(rim)

        @pl.when(me > 0)
        def _():
            rim_copy.wait_recv()

        edge = rim[...].astype(f32)
        here = pool_ref[...].astype(f32)
        window_sum = jnp.concatenate([edge, here], axis=0)
        chosen = jnp.zeros_like(here)
        for k in range(level_count):
            window_sum = window_sum + pltpu.roll(window_sum, 1 << k, 0)
            chosen = jnp.where(level == k, window_sum[MAX_WINDOW:], chosen)
        window = (2 << level).astype(f32) if hasattr(level, "astype") else float(2 << level)
        position = me * length + lax.broadcasted_iota(jnp.int32, here.shape, 0)
        counts = jnp.minimum(position.astype(f32) + 1.0, window)
        pooled = (chosen / counts - here).astype(bf16)
        mixed = dot(pooled, pool_w_ref[0]) * pool_s_ref[...]
        mix[0] = mixed.astype(bf16)

    pooling()
    partner = 2 * chip + other
    pool_mix_copy = remote(
        mix.at[0], mix.at[1], mix_send.at[0], mix_recv.at[0], tp=partner
    )

    low = me < wrapped
    down_base = jnp.where(low, me - LAG, me - n_sp - 1)
    down_first = jnp.where(low, me + 1, 0)
    down_last = jnp.where(low, wrapped - 1, me - hops - 1)
    up_steps = jnp.minimum(me, hops)

    def ring_step(step, carry):
        slot_up = jnp.maximum(me - step, 0)
        slot_down = jnp.clip(down_base + step, 0, wrapped - 1)
        takes_up = step <= up_steps
        takes_down = jnp.logical_and(
            down_base + step >= down_first, down_base + step <= down_last
        )
        for kind in range(3):

            @pl.when(takes_up)
            def _():
                up_copy(kind, slot_up, step - 1).wait_recv()

            @pl.when(jnp.logical_and(takes_up, jnp.logical_and(step < hops, me < last)))
            def _():
                up_copy(kind, slot_up, step).start()

            @pl.when(takes_down)
            def _():
                down_copy(kind, slot_down).wait_recv()

            @pl.when(jnp.logical_and(takes_down, jnp.logical_or(low, slot_down < down_last)))
            def _():
                down_copy(kind, slot_down).start()

        @pl.when(takes_up)
        def _():
            attend(slot_up)

        @pl.when(jnp.logical_and(takes_down, me > hops))
        def _():
            attend(slot_down)

        return carry

    steps = jnp.where(
        me == 0, 0, jnp.maximum(up_steps, jnp.where(low, wrapped - 1 - me + LAG, 0))
    )
    first_steps = jnp.minimum(steps, 1)
    lax.fori_loop(1, first_steps + 1, ring_step, 0)

    pool_mix_copy.start()
    load_att.wait()
    load_pool.wait()
    att_w_copy.wait_recv()
    pool_w_copy.wait_recv()
    pool_mix_copy.wait_recv()
    for c in range(CHUNKS):
        span = pl.ds(c * cols, cols)
        pool_part[:, span] = dot(mix[0], w_pool[0, :, span]) + dot(mix[1], w_pool[1, :, span])

    lax.fori_loop(first_steps + 1, steps + 1, ring_step, 0)

    for h in range(heads):
        weight_sum = jnp.sum(total[h], axis=-1, keepdims=True)
        mix[2, :, h * HEAD : (h + 1) * HEAD] = (acc[h] / weight_sum).astype(bf16)
    att_mix_copy = remote(mix.at[2], mix.at[3], mix_send.at[1], mix_recv.at[1], tp=partner)
    att_mix_copy.start()
    att_mix_copy.wait_recv()

    def relay_copies(c):
        return (
            remote(
                parts.at[2 * chip_far, c],
                relay.at[0, c],
                relay_send.at[0, c],
                relay_recv.at[0, c],
                tp=2 * chip_right + core,
            ),
            remote(
                parts.at[2 * chip_far + 1, c],
                relay.at[1, c],
                relay_send.at[1, c],
                relay_recv.at[1, c],
                tp=2 * chip_left + core,
            ),
        )

    def land_copy(side, target_chip, target_core, c):
        target = 2 * target_chip + target_core
        return remote(
            parts.at[target, c],
            landed.at[side, core, c],
            land_send.at[side, target_core, c],
            land_recv.at[side, core, c],
            tp=target,
        )

    def home_copy(c):
        return remote(
            parts.at[partner, c],
            landed.at[2, core, c],
            land_send.at[2, 0, c],
            land_recv.at[2, core, c],
            tp=partner,
        )

    for c in range(CHUNKS):
        span = pl.ds(c * cols, cols)
        part = (
            dot(mix[2], w_att[0, :, span])
            + dot(mix[3], w_att[1, :, span])
            + pool_part[:, span]
        ).astype(bf16)
        for d in range(n_tp):
            parts[d, c] = part[d * rows : (d + 1) * rows]
        for copy in relay_copies(c):
            copy.start()
    for c in range(CHUNKS):
        land_copy(0, chip_right, 1, c).start()
        land_copy(1, chip_left, 0, c).start()
    for c in range(CHUNKS):
        home_copy(c).start()
    for c in range(CHUNKS):
        from_left, from_right = relay_copies(c)
        for side, copy, target in (
            (0, from_left, 2 * chip_right),
            (1, from_right, 2 * chip_left + 1),
        ):
            copy.wait_recv()
            joined = parts[target, c].astype(f32) + relay[side, c].astype(f32)
            parts[target, c] = joined.astype(bf16)
        land_copy(0, chip_right, 0, c).start()
        land_copy(1, chip_left, 1, c).start()

    def landed_wait(side, source_core, c):
        remote(
            landed.at[side, source_core, c],
            landed.at[side, source_core, c],
            land_send.at[side, 0, c],
            land_recv.at[side, source_core, c],
            tp=partner,
        ).wait_recv()

    for c in range(CHUNKS):
        landed_wait(2, other, c)
        for source_core in range(2):
            landed_wait(0, source_core, c)
            landed_wait(1, source_core, c)
        for source_core in range(2):
            home = jnp.where(
                core == source_core,
                parts[tp, c].astype(f32),
                landed[2, source_core, c].astype(f32),
            )
            merged = (
                home
                + landed[0, source_core, c].astype(f32)
                + landed[1, source_core, c].astype(f32)
            )
            first = source_core * half + c * cols
            out_ref[:, first : first + cols] = merged.astype(bf16)

    @pl.when(me == 0)
    def _():
        pl.semaphore_wait(ready_sem, 1)
        for kind in range(3):
            down_copy(kind, 0).start()

        def pass_on(slot, carry):
            for kind in range(3):
                down_copy(kind, slot).wait_recv()
                down_copy(kind, slot).start()
            return carry

        lax.fori_loop(1, wrapped, pass_on, 0)

    @pl.when(me < last)
    def _():
        def up_sent(step, carry):
            for kind in range(3):
                up_copy(kind, me, step).wait_send()
            return carry

        lax.fori_loop(0, jnp.minimum(me, hops - 1) + 1, up_sent, 0)
        rim_copy.wait_send()

    def down_sent(slot, carry):
        for kind in range(3):
            down_copy(kind, slot).wait_send()
        return carry

    lax.fori_loop(
        jnp.where(low, me, 0), jnp.where(low, wrapped, jnp.maximum(me - hops - 1, 0)), down_sent, 0
    )
    att_w_copy.wait_send()
    pool_w_copy.wait_send()
    pool_mix_copy.wait_send()
    att_mix_copy.wait_send()
    for c in range(CHUNKS):
        for copy in relay_copies(c):
            copy.wait_send()
        land_copy(0, chip_right, 1, c).wait_send()
        land_copy(1, chip_left, 0, c).wait_send()
        land_copy(0, chip_right, 0, c).wait_send()
        land_copy(1, chip_left, 1, c).wait_send()
        home_copy(c).wait_send()


def body(
    n_sp,
    n_tp,
    query_rows,
    key_rows,
    value_rows,
    pool_input,
    log_gate_sums,
    query_gain,
    key_gain,
    pool_weight,
    pool_scale,
    attention_out,
    pooling_out,
):
    length = query_rows.shape[0]
    heads = query_rows.shape[1] // HEAD
    group = pool_input.shape[1]
    width = attention_out.shape[1]
    half = width // 2
    cols = half // CHUNKS
    rows = length // n_tp
    gate_rows = log_gate_sums.T.reshape(-1, LANES)
    gate_rows = jnp.pad(gate_rows, ((0, -gate_rows.shape[0] % 8), (0, 0)))
    wrapped = min(WRAPPED, (n_sp - 1) // 2)
    hops = n_sp - 1 - wrapped
    vmem = pl.BlockSpec(memory_space=pltpu.VMEM)
    dma = pltpu.SemaphoreType.DMA
    return pl.pallas_call(
        functools.partial(kernel, n_sp, n_tp),
        out_shape=jax.ShapeDtypeStruct((rows, width), bf16),
        in_specs=[vmem] * 9 + [pl.BlockSpec(memory_space=pl.ANY)] * 2,
        out_specs=vmem,
        scratch_shapes=[
            pltpu.VMEM((n_sp, length, HEAD), bf16),
            pltpu.VMEM((n_sp, length, HEAD), bf16),
            pltpu.VMEM((n_sp,) + gate_rows.shape, f32),
            pltpu.VMEM((heads, length, HEAD), bf16),
            pltpu.VMEM((heads, length, LANES), f32),
            pltpu.VMEM((heads, length, LANES), f32),
            pltpu.VMEM((heads, length, HEAD), f32),
            pltpu.VMEM((4, length, group), bf16),
            pltpu.VMEM((MAX_WINDOW, group), bf16),
            pltpu.VMEM((2, heads * HEAD, half), bf16),
            pltpu.VMEM((2, group, half), bf16),
            pltpu.VMEM((length, half), f32),
            pltpu.VMEM((n_tp, CHUNKS, rows, cols), bf16),
            pltpu.VMEM((2, CHUNKS, rows, cols), bf16),
            pltpu.VMEM((3, 2, CHUNKS, rows, cols), bf16),
            dma((3, hops)),
            dma((3, hops)),
            dma((3, wrapped)),
            dma((3, wrapped)),
            pltpu.SemaphoreType.REGULAR,
            dma((3,)),
            dma((3,)),
            dma((2,)),
            dma((2,)),
            dma((2,)),
            dma((2, CHUNKS)),
            dma((2, CHUNKS)),
            dma((3, 2, CHUNKS)),
            dma((3, 2, CHUNKS)),
        ],
        compiler_params=pltpu.CompilerParams(
            collective_id=0, has_side_effects=True, vmem_limit_bytes=56 * 1024 * 1024
        ),
    )(
        query_rows,
        key_rows,
        value_rows,
        gate_rows,
        pool_input,
        query_gain.reshape(1, -1),
        key_gain.reshape(1, -1),
        pool_weight,
        pool_scale.reshape(1, -1),
        attention_out,
        pooling_out,
    )


def solution(mesh):
    return jax.shard_map(
        functools.partial(body, mesh.shape["sp"], mesh.shape["tp"]),
        mesh=mesh,
        in_specs=(
            P(("grp", "sp"), "tp"),
            P(("grp", "sp"), "tp"),
            P(("grp", "sp"), "tp"),
            P(("grp", "sp"), "tp"),
            P(("grp", "sp"), "tp"),
            P(),
            P(),
            P("tp", None, None),
            P("tp"),
            P("tp", None),
            P("tp", None),
        ),
        out_specs=P(("grp", "sp", "tp"), None),
        check_vma=False,
    )
```

```python
import functools
import math

import jax
import jax.numpy as jnp
from jax import lax
from jax.experimental import pallas as pl
from jax.experimental.pallas import tpu as pltpu
from jax.sharding import PartitionSpec as P

HEAD = 128
MAX_WINDOW = 16
LANES = 128
CHUNKS = 4
WRAPPED = 15
AHEAD = 4
SEND_STEP = 11

epsilon = 1e-06
masked = -1e30
LOG2E = math.log2(math.e)

f32 = jnp.float32
bf16 = jnp.bfloat16


def normed(rows, gain):
    wide = rows.astype(f32)
    scale = lax.rsqrt(jnp.mean(wide * wide, axis=-1, keepdims=True) + epsilon)
    return (wide * scale * gain).astype(bf16)


def rows_dot(a, b):
    return lax.dot_general(a, b, (((1,), (1,)), ((), ())), preferred_element_type=f32)


def dot(a, b):
    return jnp.dot(a, b, preferred_element_type=f32)


def kernel(
    n_sp,
    n_tp,
    q_ref,
    k_ref,
    v_ref,
    gate_ref,
    pool_ref,
    q_gain_ref,
    k_gain_ref,
    pool_w_ref,
    pool_s_ref,
    att_w_hbm,
    pool_w_out_hbm,
    out_ref,
    keys,
    values,
    gates,
    queries,
    best,
    total,
    acc,
    mix,
    rim,
    w_att,
    w_pool,
    pool_part,
    parts,
    relay,
    landed,
    up_send,
    up_recv,
    down_send,
    down_recv,
    ready_sem,
    early_send,
    early_recv,
    local_sem,
    mix_send,
    mix_recv,
    relay_send,
    relay_recv,
    land_send,
    land_recv,
):
    me = lax.axis_index("sp")
    tp = lax.axis_index("tp")
    length = q_ref.shape[0]
    heads = q_ref.shape[1] // HEAD
    pieces = length // LANES
    n_x = n_tp // 2
    core = lax.rem(tp, 2)
    other = 1 - core
    chip = tp // 2
    chip_right = lax.rem(chip + 1, n_x)
    chip_left = lax.rem(chip + n_x - 1, n_x)
    chip_far = lax.rem(chip + 2, n_x)
    above = lax.rem(me + 1, n_sp)
    below = lax.rem(me + n_sp - 1, n_sp)
    wrapped = min(WRAPPED, (n_sp - 1) // 2)
    hops = n_sp - 1 - wrapped
    last = n_sp - 1
    half = out_ref.shape[1] // 2
    cols = half // CHUNKS
    rows = out_ref.shape[0]

    def remote(src, dst, send_sem, recv_sem, **where):
        return pltpu.make_async_remote_copy(
            src_ref=src,
            dst_ref=dst,
            send_sem=send_sem,
            recv_sem=recv_sem,
            device_id=where,
            device_id_type=pl.DeviceIdType.MESH,
        )

    barrier = pltpu.get_barrier_semaphore()
    @pl.when(me < last)
    def _():
        pl.semaphore_signal(
            barrier, inc=1, device_id={"sp": above}, device_id_type=pl.DeviceIdType.MESH
        )

    @pl.when(jnp.logical_and(me > 0, me < wrapped))
    def _():
        pl.semaphore_signal(
            barrier, inc=1, device_id={"sp": last}, device_id_type=pl.DeviceIdType.MESH
        )

    for where in (
        {"sp": below},
        {"tp": 2 * chip + other},
        {"tp": 2 * chip_right},
        {"tp": 2 * chip_right + 1},
        {"tp": 2 * chip_left},
        {"tp": 2 * chip_left + 1},
    ):
        pl.semaphore_signal(
            barrier, inc=1, device_id=where, device_id_type=pl.DeviceIdType.MESH
        )

    my_cols = pl.ds(pl.multiple_of(core * half, LANES), half)
    other_cols = pl.ds(pl.multiple_of(other * half, LANES), half)
    load_att = pltpu.make_async_copy(att_w_hbm.at[:, my_cols], w_att.at[0], local_sem.at[0])
    load_pool = pltpu.make_async_copy(
        pool_w_out_hbm.at[:, my_cols], w_pool.at[0], local_sem.at[1]
    )
    load_att.start()
    load_pool.start()

    keys[me] = normed(k_ref[...], k_gain_ref[...])
    values[me] = v_ref[...]
    gates[me] = jnp.concatenate(
        [
            gate_ref[h : h + 1, c * LANES : (c + 1) * LANES]
            for h in range(heads)
            for c in range(pieces)
        ]
        + [jnp.zeros((-(heads * pieces) % 8, LANES), f32)],
        axis=0,
    )
    for h in range(heads):
        queries[h] = normed(q_ref[:, h * HEAD : (h + 1) * HEAD], q_gain_ref[...])

    @pl.when(me == 0)
    def _():
        pl.semaphore_wait(barrier, 6)

    @pl.when(jnp.logical_and(me > 0, me < last))
    def _():
        pl.semaphore_wait(barrier, 7)

    def let_send(plane):
        pl.semaphore_signal(
            ready_sem, inc=1, device_id={"sp": plane}, device_id_type=pl.DeviceIdType.MESH
        )

    @pl.when(me == last)
    def _():
        pl.semaphore_wait(barrier, 6 + wrapped)
        for plane in range(min(AHEAD, wrapped)):
            let_send(plane)

    stores = (values, gates, keys)

    def up_copy(kind, slot, step):
        return remote(
            stores[kind].at[slot],
            stores[kind].at[slot],
            up_send.at[kind, step],
            up_recv.at[kind, step],
            sp=above,
        )

    def down_copy(kind, slot, plane):
        return remote(
            stores[kind].at[slot],
            stores[kind].at[slot],
            down_send.at[kind, slot],
            down_recv.at[kind, slot],
            sp=plane,
        )

    @pl.when(me < last)
    def _():
        for kind in range(3):
            up_copy(kind, me, 0).start()

    rim_copy = remote(
        pool_ref.at[pl.ds(length - MAX_WINDOW, MAX_WINDOW)],
        rim,
        early_send.at[0],
        early_recv.at[0],
        sp=above,
    )
    att_w_copy = remote(
        att_w_hbm.at[:, other_cols],
        w_att.at[1],
        early_send.at[1],
        early_recv.at[1],
        tp=2 * chip + other,
    )
    pool_w_copy = remote(
        pool_w_out_hbm.at[:, other_cols],
        w_pool.at[1],
        early_send.at[2],
        early_recv.at[2],
        tp=2 * chip + other,
    )

    @pl.when(me < last)
    def _():
        rim_copy.start()

    att_w_copy.start()
    pool_w_copy.start()

    scale = LOG2E / math.sqrt(HEAD)

    def score_pieces(h, slot):
        z = rows_dot(queries[h], keys[slot])
        base = gate_ref[h : h + 1, 0:1]
        lifted = (base - gates[slot]) * LOG2E
        return [
            z[:, c * LANES : (c + 1) * LANES] * scale
            + lifted[h * pieces + c : h * pieces + c + 1, :]
            for c in range(pieces)
        ]

    def row_max(score):
        most = functools.reduce(jnp.maximum, score)
        return jnp.max(most, axis=-1, keepdims=True)

    def weigh(score, top):
        weights = [jnp.exp2(s - top) for s in score]
        return functools.reduce(jnp.add, weights), jnp.concatenate(
            [w.astype(bf16) for w in weights], axis=1
        )

    def attend_own():
        for h in range(heads):
            score = score_pieces(h, me)
            position = lax.broadcasted_iota(jnp.int32, (length, LANES), 0)
            lane = lax.broadcasted_iota(jnp.int32, (length, LANES), 1)
            score = [
                jnp.where(lane + c * LANES <= position, s, masked) for c, s in enumerate(score)
            ]
            top = jnp.broadcast_to(row_max(score), (length, LANES))
            summed, weights = weigh(score, top)
            best[h] = top
            total[h] = summed
            acc[h] = dot(weights, values[me])

    def attend(slot):
        for h in range(heads):
            score = score_pieces(h, slot)
            before = best[h]
            top = jnp.maximum(before, row_max(score))
            fade = jnp.exp2(before - top)
            summed, weights = weigh(score, top)
            best[h] = top
            total[h] = total[h] * fade + summed
            acc[h] = acc[h] * fade + dot(weights, values[slot])

    attend_own()

    level_count = MAX_WINDOW.bit_length() - 1
    level = lax.rem(tp, level_count)

    def pooling():
        @pl.when(me == 0)
        def _():
            rim[...] = jnp.zeros_like(rim)

        @pl.when(me > 0)
        def _():
            rim_copy.wait_recv()

        edge = rim[...].astype(f32)
        here = pool_ref[...].astype(f32)
        window_sum = jnp.concatenate([edge, here], axis=0)
        chosen = jnp.zeros_like(here)
        for k in range(level_count):
            window_sum = window_sum + pltpu.roll(window_sum, 1 << k, 0)
            chosen = jnp.where(level == k, window_sum[MAX_WINDOW:], chosen)
        window = (2 << level).astype(f32) if hasattr(level, "astype") else float(2 << level)
        position = me * length + lax.broadcasted_iota(jnp.int32, here.shape, 0)
        counts = jnp.minimum(position.astype(f32) + 1.0, window)
        pooled = (chosen / counts - here).astype(bf16)
        mixed = dot(pooled, pool_w_ref[0]) * pool_s_ref[...]
        mix[0] = mixed.astype(bf16)

    pooling()
    partner = 2 * chip + other
    pool_mix_copy = remote(
        mix.at[0], mix.at[1], mix_send.at[0], mix_recv.at[0], tp=partner
    )

    low = me < wrapped
    own_slot = jnp.minimum(me, wrapped - 1)
    down_base = me - n_sp - 1
    down_last = me - hops - 1
    up_steps = jnp.minimum(me, hops)
    send_step = jnp.minimum(me, SEND_STEP)

    def send_across():
        pl.semaphore_wait(ready_sem, 1)
        for kind in range(3):
            down_copy(kind, own_slot, last).start()

    def has_down(step):
        return jnp.logical_and(down_base + step >= 0, down_base + step <= down_last)

    def ring_step(step, carry):
        slot_up = jnp.maximum(me - step, 0)
        slot_down = jnp.clip(down_base + step, 0, wrapped - 1)
        takes_up = step <= up_steps
        takes_down = has_down(step)

        def pass_on(kind):
            @pl.when(takes_up)
            def _():
                up_copy(kind, slot_up, step - 1).wait_recv()

            @pl.when(jnp.logical_and(takes_up, jnp.logical_and(step < hops, me < last)))
            def _():
                up_copy(kind, slot_up, step).start()

            @pl.when(takes_down)
            def _():
                down_copy(kind, slot_down, below).wait_recv()

            @pl.when(jnp.logical_and(takes_down, slot_down < down_last))
            def _():
                down_copy(kind, slot_down, below).start()

        pass_on(0)
        pass_on(1)

        @pl.when(jnp.logical_and(step > 1, step - 1 <= up_steps))
        def _():
            attend(jnp.maximum(me - step + 1, 0))

        pass_on(2)

        @pl.when(jnp.logical_and(me == last, takes_down))
        def _():
            for ahead in range(2):
                plane = 2 * slot_down + AHEAD + ahead

                @pl.when(plane < wrapped)
                def _():
                    let_send(plane)

        @pl.when(has_down(step - 1))
        def _():
            attend(jnp.clip(down_base + step - 1, 0, wrapped - 1))

        @pl.when(jnp.logical_and(low, step == send_step))
        def _():
            send_across()

        return carry

    steps = jnp.where(me == 0, 0, up_steps + 1)
    first_steps = jnp.minimum(steps, 1)
    lax.fori_loop(1, first_steps + 1, ring_step, 0)

    pool_mix_copy.start()
    load_att.wait()
    load_pool.wait()
    att_w_copy.wait_recv()
    pool_w_copy.wait_recv()
    pool_mix_copy.wait_recv()
    for c in range(CHUNKS):
        span = pl.ds(c * cols, cols)
        pool_part[:, span] = dot(mix[0], w_pool[0, :, span]) + dot(mix[1], w_pool[1, :, span])

    lax.fori_loop(first_steps + 1, steps + 1, ring_step, 0)

    @pl.when(me == 0)
    def _():
        send_across()

    for h in range(heads):
        weight_sum = jnp.sum(total[h], axis=-1, keepdims=True)
        mix[2, :, h * HEAD : (h + 1) * HEAD] = (acc[h] / weight_sum).astype(bf16)
    att_mix_copy = remote(mix.at[2], mix.at[3], mix_send.at[1], mix_recv.at[1], tp=partner)
    att_mix_copy.start()
    att_mix_copy.wait_recv()

    def relay_copies(c):
        return (
            remote(
                parts.at[2 * chip_far, c],
                relay.at[0, c],
                relay_send.at[0, c],
                relay_recv.at[0, c],
                tp=2 * chip_right + core,
            ),
            remote(
                parts.at[2 * chip_far + 1, c],
                relay.at[1, c],
                relay_send.at[1, c],
                relay_recv.at[1, c],
                tp=2 * chip_left + core,
            ),
        )

    def land_copy(side, target_chip, target_core, c):
        target = 2 * target_chip + target_core
        return remote(
            parts.at[target, c],
            landed.at[side, core, c],
            land_send.at[side, target_core, c],
            land_recv.at[side, core, c],
            tp=target,
        )

    def home_copy(c):
        return remote(
            parts.at[partner, c],
            landed.at[2, core, c],
            land_send.at[2, 0, c],
            land_recv.at[2, core, c],
            tp=partner,
        )

    for c in range(CHUNKS):
        span = pl.ds(c * cols, cols)
        part = (
            dot(mix[2], w_att[0, :, span])
            + dot(mix[3], w_att[1, :, span])
            + pool_part[:, span]
        ).astype(bf16)
        for d in range(n_tp):
            parts[d, c] = part[d * rows : (d + 1) * rows]
        for copy in relay_copies(c):
            copy.start()
    for c in range(CHUNKS):
        land_copy(0, chip_right, 1, c).start()
        land_copy(1, chip_left, 0, c).start()
    for c in range(CHUNKS):
        home_copy(c).start()
    for c in range(CHUNKS):
        from_left, from_right = relay_copies(c)
        for side, copy, target in (
            (0, from_left, 2 * chip_right),
            (1, from_right, 2 * chip_left + 1),
        ):
            copy.wait_recv()
            joined = parts[target, c].astype(f32) + relay[side, c].astype(f32)
            parts[target, c] = joined.astype(bf16)
        land_copy(0, chip_right, 0, c).start()
        land_copy(1, chip_left, 1, c).start()

    def landed_wait(side, source_core, c):
        remote(
            landed.at[side, source_core, c],
            landed.at[side, source_core, c],
            land_send.at[side, 0, c],
            land_recv.at[side, source_core, c],
            tp=partner,
        ).wait_recv()

    for c in range(CHUNKS):
        landed_wait(2, other, c)
        for source_core in range(2):
            landed_wait(0, source_core, c)
            landed_wait(1, source_core, c)
        for source_core in range(2):
            home = jnp.where(
                core == source_core,
                parts[tp, c].astype(f32),
                landed[2, source_core, c].astype(f32),
            )
            merged = (
                home
                + landed[0, source_core, c].astype(f32)
                + landed[1, source_core, c].astype(f32)
            )
            first = source_core * half + c * cols
            out_ref[:, first : first + cols] = merged.astype(bf16)

    @pl.when(me < last)
    def _():
        def up_sent(step, carry):
            for kind in range(3):
                up_copy(kind, me, step).wait_send()
            return carry

        lax.fori_loop(0, jnp.minimum(me, hops - 1) + 1, up_sent, 0)
        rim_copy.wait_send()

    def down_sent(slot, carry):
        for kind in range(3):
            down_copy(kind, slot, below).wait_send()
        return carry

    lax.fori_loop(
        jnp.where(low, own_slot, 0),
        jnp.where(low, own_slot + 1, jnp.maximum(me - hops - 1, 0)),
        down_sent,
        0,
    )
    att_w_copy.wait_send()
    pool_w_copy.wait_send()
    pool_mix_copy.wait_send()
    att_mix_copy.wait_send()
    for c in range(CHUNKS):
        for copy in relay_copies(c):
            copy.wait_send()
        land_copy(0, chip_right, 1, c).wait_send()
        land_copy(1, chip_left, 0, c).wait_send()
        land_copy(0, chip_right, 0, c).wait_send()
        land_copy(1, chip_left, 1, c).wait_send()
        home_copy(c).wait_send()


def body(
    n_sp,
    n_tp,
    query_rows,
    key_rows,
    value_rows,
    pool_input,
    log_gate_sums,
    query_gain,
    key_gain,
    pool_weight,
    pool_scale,
    attention_out,
    pooling_out,
):
    length = query_rows.shape[0]
    heads = query_rows.shape[1] // HEAD
    group = pool_input.shape[1]
    width = attention_out.shape[1]
    half = width // 2
    cols = half // CHUNKS
    rows = length // n_tp
    gate_tile = -(-heads * length // LANES // 8) * 8
    wrapped = min(WRAPPED, (n_sp - 1) // 2)
    hops = n_sp - 1 - wrapped
    vmem = pl.BlockSpec(memory_space=pltpu.VMEM)
    dma = pltpu.SemaphoreType.DMA
    return pl.pallas_call(
        functools.partial(kernel, n_sp, n_tp),
        out_shape=jax.ShapeDtypeStruct((rows, width), bf16),
        in_specs=[vmem] * 9 + [pl.BlockSpec(memory_space=pl.ANY)] * 2,
        out_specs=vmem,
        scratch_shapes=[
            pltpu.VMEM((n_sp, length, HEAD), bf16),
            pltpu.VMEM((n_sp, length, HEAD), bf16),
            pltpu.VMEM((n_sp, gate_tile, LANES), f32),
            pltpu.VMEM((heads, length, HEAD), bf16),
            pltpu.VMEM((heads, length, LANES), f32),
            pltpu.VMEM((heads, length, LANES), f32),
            pltpu.VMEM((heads, length, HEAD), f32),
            pltpu.VMEM((4, length, group), bf16),
            pltpu.VMEM((MAX_WINDOW, group), bf16),
            pltpu.VMEM((2, heads * HEAD, half), bf16),
            pltpu.VMEM((2, group, half), bf16),
            pltpu.VMEM((length, half), f32),
            pltpu.VMEM((n_tp, CHUNKS, rows, cols), bf16),
            pltpu.VMEM((2, CHUNKS, rows, cols), bf16),
            pltpu.VMEM((3, 2, CHUNKS, rows, cols), bf16),
            dma((3, hops)),
            dma((3, hops)),
            dma((3, wrapped)),
            dma((3, wrapped)),
            pltpu.SemaphoreType.REGULAR,
            dma((3,)),
            dma((3,)),
            dma((2,)),
            dma((2,)),
            dma((2,)),
            dma((2, CHUNKS)),
            dma((2, CHUNKS)),
            dma((3, 2, CHUNKS)),
            dma((3, 2, CHUNKS)),
        ],
        compiler_params=pltpu.CompilerParams(
            collective_id=0, has_side_effects=True, vmem_limit_bytes=56 * 1024 * 1024
        ),
    )(
        query_rows,
        key_rows,
        value_rows,
        log_gate_sums.T,
        pool_input,
        query_gain.reshape(1, -1),
        key_gain.reshape(1, -1),
        pool_weight,
        pool_scale.reshape(1, -1),
        attention_out,
        pooling_out,
    )


def solution(mesh):
    return jax.shard_map(
        functools.partial(body, mesh.shape["sp"], mesh.shape["tp"]),
        mesh=mesh,
        in_specs=(
            P(("grp", "sp"), "tp"),
            P(("grp", "sp"), "tp"),
            P(("grp", "sp"), "tp"),
            P(("grp", "sp"), "tp"),
            P(("grp", "sp"), "tp"),
            P(),
            P(),
            P("tp", None, None),
            P("tp"),
            P("tp", None),
            P("tp", None),
        ),
        out_specs=P(("grp", "sp", "tp"), None),
        check_vma=False,
    )
```

```python
import functools
import math

import jax
import jax.numpy as jnp
from jax import lax
from jax.experimental import pallas as pl
from jax.experimental.pallas import tpu as pltpu
from jax.sharding import PartitionSpec as P

HEAD = 128
MAX_WINDOW = 16
LANES = 128
CHUNKS = 4
WRAPPED = 13
LAG = 3
UPPER_LAG = 3
SOON_FIRST = 2
SOON = 5

epsilon = 1e-06
masked = -1e30
LOG2E = math.log2(math.e)

f32 = jnp.float32
bf16 = jnp.bfloat16


def normed(rows, gain):
    wide = rows.astype(f32)
    scale = lax.rsqrt(jnp.mean(wide * wide, axis=-1, keepdims=True) + epsilon)
    return (wide * scale * gain).astype(bf16)


def rows_dot(a, b):
    return lax.dot_general(a, b, (((1,), (1,)), ((), ())), preferred_element_type=f32)


def dot(a, b):
    return jnp.dot(a, b, preferred_element_type=f32)


def kernel(
    n_sp,
    n_tp,
    q_ref,
    k_ref,
    v_ref,
    gate_ref,
    pool_ref,
    q_gain_ref,
    k_gain_ref,
    pool_w_ref,
    pool_s_ref,
    att_w_hbm,
    pool_w_out_hbm,
    out_ref,
    keys,
    values,
    gates,
    queries,
    best,
    total,
    acc,
    mix,
    rim,
    w_att,
    w_pool,
    pool_part,
    parts,
    relay,
    landed,
    up_send,
    up_recv,
    down_send,
    down_recv,
    ready_sem,
    late_sem,
    early_send,
    early_recv,
    local_sem,
    mix_send,
    mix_recv,
    relay_send,
    relay_recv,
    land_send,
    land_recv,
):
    me = lax.axis_index("sp")
    tp = lax.axis_index("tp")
    length = q_ref.shape[0]
    heads = q_ref.shape[1] // HEAD
    pieces = length // LANES
    n_x = n_tp // 2
    core = lax.rem(tp, 2)
    other = 1 - core
    chip = tp // 2
    chip_right = lax.rem(chip + 1, n_x)
    chip_left = lax.rem(chip + n_x - 1, n_x)
    chip_far = lax.rem(chip + 2, n_x)
    above = lax.rem(me + 1, n_sp)
    below = lax.rem(me + n_sp - 1, n_sp)
    wrapped = min(WRAPPED, (n_sp - 1) // 2)
    hops = n_sp - 1 - wrapped
    last = n_sp - 1
    half = out_ref.shape[1] // 2
    cols = half // CHUNKS
    rows = out_ref.shape[0]

    def remote(src, dst, send_sem, recv_sem, **where):
        return pltpu.make_async_remote_copy(
            src_ref=src,
            dst_ref=dst,
            send_sem=send_sem,
            recv_sem=recv_sem,
            device_id=where,
            device_id_type=pl.DeviceIdType.MESH,
        )

    barrier = pltpu.get_barrier_semaphore()
    first = jnp.logical_and(me == 0, tp == 0)
    beside_z = jnp.logical_and(tp == 0, me == 1)
    beside_chip = jnp.logical_or(chip == 1, chip == n_x - 1)
    beside_x = jnp.logical_and(me == 0, jnp.logical_or(tp == 1, beside_chip))
    beside = jnp.logical_or(beside_z, beside_x)

    def signal(sem, where):
        pl.semaphore_signal(
            sem, inc=1, device_id=where, device_id_type=pl.DeviceIdType.MESH
        )

    neighbours = (
        {"tp": 2 * chip + other},
        {"tp": 2 * chip_right},
        {"tp": 2 * chip_right + 1},
        {"tp": 2 * chip_left},
        {"tp": 2 * chip_left + 1},
    )

    signal(barrier, {"sp": below})

    @pl.when(jnp.logical_not(first))
    def _():
        @pl.when(me < last)
        def _():
            signal(barrier, {"sp": above})

        for where in neighbours:
            signal(barrier, where)

    my_cols = pl.ds(pl.multiple_of(core * half, LANES), half)
    other_cols = pl.ds(pl.multiple_of(other * half, LANES), half)
    load_att = pltpu.make_async_copy(att_w_hbm.at[:, my_cols], w_att.at[0], local_sem.at[0])
    load_pool = pltpu.make_async_copy(
        pool_w_out_hbm.at[:, my_cols], w_pool.at[0], local_sem.at[1]
    )
    load_att.start()
    load_pool.start()

    keys[me] = normed(k_ref[...], k_gain_ref[...])
    values[me] = v_ref[...]
    gates[me] = jnp.concatenate(
        [
            gate_ref[h : h + 1, c * LANES : (c + 1) * LANES]
            for h in range(heads)
            for c in range(pieces)
        ]
        + [jnp.zeros((-(heads * pieces) % 8, LANES), f32)],
        axis=0,
    )
    for h in range(heads):
        queries[h] = normed(q_ref[:, h * HEAD : (h + 1) * HEAD], q_gain_ref[...])

    arrivals = 7 - jnp.where(me == 0, 1, 0) - jnp.where(beside, 1, 0)
    pl.semaphore_wait(barrier, arrivals)

    @pl.when(first)
    def _():
        signal(late_sem, {"sp": above})
        for where in neighbours:
            signal(late_sem, where)

    @pl.when(me == last)
    def _():
        signal(ready_sem, {"sp": above})

    stores = (values, gates, keys)

    def up_copy(kind, slot, step):
        return remote(
            stores[kind].at[slot],
            stores[kind].at[slot],
            up_send.at[kind, step],
            up_recv.at[kind, step],
            sp=above,
        )

    def down_copy(kind, slot):
        return remote(
            stores[kind].at[slot],
            stores[kind].at[slot],
            down_send.at[kind, slot],
            down_recv.at[kind, slot],
            sp=below,
        )

    @pl.when(me < last)
    def _():
        for kind in range(3):
            up_copy(kind, me, 0).start()

    def start_down():
        for kind in range(3):
            down_copy(kind, me).start()

    starts_down = jnp.logical_and(me > 0, me < wrapped)

    @pl.when(jnp.logical_and(starts_down, jnp.logical_not(beside)))
    def _():
        start_down()

    rim_copy = remote(
        pool_ref.at[pl.ds(length - MAX_WINDOW, MAX_WINDOW)],
        rim,
        early_send.at[0],
        early_recv.at[0],
        sp=above,
    )
    att_w_copy = remote(
        att_w_hbm.at[:, other_cols],
        w_att.at[1],
        early_send.at[1],
        early_recv.at[1],
        tp=2 * chip + other,
    )
    pool_w_copy = remote(
        pool_w_out_hbm.at[:, other_cols],
        w_pool.at[1],
        early_send.at[2],
        early_recv.at[2],
        tp=2 * chip + other,
    )

    @pl.when(me < last)
    def _():
        rim_copy.start()

    scale = LOG2E / math.sqrt(HEAD)

    def score_pieces(h, slot):
        z = rows_dot(queries[h], keys[slot])
        base = gate_ref[h : h + 1, 0:1]
        lifted = (base - gates[slot]) * LOG2E
        return [
            z[:, c * LANES : (c + 1) * LANES] * scale
            + lifted[h * pieces + c : h * pieces + c + 1, :]
            for c in range(pieces)
        ]

    def row_max(score):
        most = functools.reduce(jnp.maximum, score)
        return jnp.max(most, axis=-1, keepdims=True)

    def weigh(score, top):
        weights = [jnp.exp2(s - top) for s in score]
        return functools.reduce(jnp.add, weights), jnp.concatenate(
            [w.astype(bf16) for w in weights], axis=1
        )

    def attend_own():
        for h in range(heads):
            score = score_pieces(h, me)
            position = lax.broadcasted_iota(jnp.int32, (length, LANES), 0)
            lane = lax.broadcasted_iota(jnp.int32, (length, LANES), 1)
            score = [
                jnp.where(lane + c * LANES <= position, s, masked) for c, s in enumerate(score)
            ]
            top = jnp.broadcast_to(row_max(score), (length, LANES))
            summed, weights = weigh(score, top)
            best[h] = top
            total[h] = summed
            acc[h] = dot(weights, values[me])

    def attend(slot):
        for h in range(heads):
            score = score_pieces(h, slot)
            before = best[h]
            top = jnp.maximum(before, row_max(score))
            fade = jnp.exp2(before - top)
            summed, weights = weigh(score, top)
            best[h] = top
            total[h] = total[h] * fade + summed
            acc[h] = acc[h] * fade + dot(weights, values[slot])

    attend_own()

    level_count = MAX_WINDOW.bit_length() - 1
    level = lax.rem(tp, level_count)

    def pooling():
        @pl.when(me == 0)
        def _():
            rim[...] = jnp.zeros_like(rim)

        @pl.when(me > 0)
        def _():
            rim_copy.wait_recv()

        edge = rim[...].astype(f32)
        here = pool_ref[...].astype(f32)
        window_sum = jnp.concatenate([edge, here], axis=0)
        chosen = jnp.zeros_like(here)
        for k in range(level_count):
            window_sum = window_sum + pltpu.roll(window_sum, 1 << k, 0)
            chosen = jnp.where(level == k, window_sum[MAX_WINDOW:], chosen)
        window = (2 << level).astype(f32) if hasattr(level, "astype") else float(2 << level)
        position = me * length + lax.broadcasted_iota(jnp.int32, here.shape, 0)
        counts = jnp.minimum(position.astype(f32) + 1.0, window)
        pooled = (chosen / counts - here).astype(bf16)
        mixed = dot(pooled, pool_w_ref[0]) * pool_s_ref[...]
        mix[0] = mixed.astype(bf16)

    pooling()

    def cross(slot, carry):
        for kind in range(3):
            down_copy(kind, slot).wait_recv()
            down_copy(kind, slot).start()
        return carry

    soon = jnp.where(first, SOON_FIRST, SOON)

    @pl.when(me == 0)
    def _():
        pl.semaphore_wait(ready_sem, 1)
        for kind in range(3):
            down_copy(kind, 0).start()
        lax.fori_loop(1, soon, cross, 0)

    @pl.when(beside)
    def _():
        pl.semaphore_wait(late_sem, 1)

        @pl.when(starts_down)
        def _():
            start_down()

    att_w_copy.start()
    pool_w_copy.start()
    partner = 2 * chip + other
    pool_mix_copy = remote(
        mix.at[0], mix.at[1], mix_send.at[0], mix_recv.at[0], tp=partner
    )

    low = me < wrapped
    down_base = jnp.where(low, me - LAG, me - n_sp + 1 - UPPER_LAG)
    down_first = jnp.where(low, me + 1, 0)
    down_last = jnp.where(low, wrapped - 1, me - hops - 1)
    up_steps = jnp.minimum(me, hops)

    def has_down(step):
        return jnp.logical_and(down_base + step >= down_first, down_base + step <= down_last)

    def ring_step(step, carry):
        slot_up = jnp.maximum(me - step, 0)
        slot_down = jnp.clip(down_base + step, 0, wrapped - 1)
        takes_up = step <= up_steps
        takes_down = has_down(step)

        def pass_on(kind):
            @pl.when(takes_up)
            def _():
                up_copy(kind, slot_up, step - 1).wait_recv()

            @pl.when(jnp.logical_and(takes_up, jnp.logical_and(step < hops, me < last)))
            def _():
                up_copy(kind, slot_up, step).start()

            @pl.when(takes_down)
            def _():
                down_copy(kind, slot_down).wait_recv()

            @pl.when(jnp.logical_and(takes_down, jnp.logical_or(low, slot_down < down_last)))
            def _():
                down_copy(kind, slot_down).start()

        pass_on(0)
        pass_on(1)

        @pl.when(jnp.logical_and(step > 1, step - 1 <= up_steps))
        def _():
            attend(jnp.maximum(me - step + 1, 0))

        pass_on(2)

        @pl.when(jnp.logical_and(me > hops, has_down(step - 1)))
        def _():
            attend(jnp.clip(down_base + step - 1, 0, wrapped - 1))

        return carry

    steps = jnp.where(
        me == 0, 0, jnp.maximum(up_steps + 1, jnp.where(low, wrapped - 1 - me + LAG, 0))
    )
    first_steps = jnp.minimum(steps, 1)
    lax.fori_loop(1, first_steps + 1, ring_step, 0)

    pool_mix_copy.start()
    load_att.wait()
    load_pool.wait()
    att_w_copy.wait_recv()
    pool_w_copy.wait_recv()
    pool_mix_copy.wait_recv()
    for c in range(CHUNKS):
        span = pl.ds(c * cols, cols)
        pool_part[:, span] = dot(mix[0], w_pool[0, :, span]) + dot(mix[1], w_pool[1, :, span])

    lax.fori_loop(first_steps + 1, steps + 1, ring_step, 0)

    for h in range(heads):
        weight_sum = jnp.sum(total[h], axis=-1, keepdims=True)
        mix[2, :, h * HEAD : (h + 1) * HEAD] = (acc[h] / weight_sum).astype(bf16)
    att_mix_copy = remote(mix.at[2], mix.at[3], mix_send.at[1], mix_recv.at[1], tp=partner)
    att_mix_copy.start()
    for c in range(CHUNKS):
        span = pl.ds(c * cols, cols)
        pool_part[:, span] += dot(mix[2], w_att[0, :, span])
    att_mix_copy.wait_recv()

    def relay_copies(c):
        return (
            remote(
                parts.at[2 * chip_far, c],
                relay.at[0, c],
                relay_send.at[0, c],
                relay_recv.at[0, c],
                tp=2 * chip_right + core,
            ),
            remote(
                parts.at[2 * chip_far + 1, c],
                relay.at[1, c],
                relay_send.at[1, c],
                relay_recv.at[1, c],
                tp=2 * chip_left + core,
            ),
        )

    def land_copy(side, target_chip, target_core, c):
        target = 2 * target_chip + target_core
        return remote(
            parts.at[target, c],
            landed.at[side, core, c],
            land_send.at[side, target_core, c],
            land_recv.at[side, core, c],
            tp=target,
        )

    def home_copy(c):
        return remote(
            parts.at[partner, c],
            landed.at[2, core, c],
            land_send.at[2, 0, c],
            land_recv.at[2, core, c],
            tp=partner,
        )

    for c in range(CHUNKS):
        span = pl.ds(c * cols, cols)
        part = (pool_part[:, span] + dot(mix[3], w_att[1, :, span])).astype(bf16)
        for d in range(n_tp):
            parts[d, c] = part[d * rows : (d + 1) * rows]
        for copy in relay_copies(c):
            copy.start()
    for c in range(CHUNKS):
        land_copy(0, chip_right, 1, c).start()
        land_copy(1, chip_left, 0, c).start()

    @pl.when(me == 0)
    def _():
        cross(soon, 0)

    for c in range(CHUNKS):
        home_copy(c).start()
    for c in range(CHUNKS):
        from_left, from_right = relay_copies(c)
        for side, copy, target in (
            (0, from_left, 2 * chip_right),
            (1, from_right, 2 * chip_left + 1),
        ):
            copy.wait_recv()
            joined = parts[target, c].astype(f32) + relay[side, c].astype(f32)
            parts[target, c] = joined.astype(bf16)
        land_copy(0, chip_right, 0, c).start()
        land_copy(1, chip_left, 1, c).start()

        @pl.when(me == 0)
        def _():
            cross(soon + 1 + c, 0)

    def landed_wait(side, source_core, c):
        remote(
            landed.at[side, source_core, c],
            landed.at[side, source_core, c],
            land_send.at[side, 0, c],
            land_recv.at[side, source_core, c],
            tp=partner,
        ).wait_recv()

    for c in range(CHUNKS):
        landed_wait(2, other, c)
        for source_core in range(2):
            landed_wait(0, source_core, c)
            landed_wait(1, source_core, c)
        for source_core in range(2):
            home = jnp.where(
                core == source_core,
                parts[tp, c].astype(f32),
                landed[2, source_core, c].astype(f32),
            )
            merged = (
                home
                + landed[0, source_core, c].astype(f32)
                + landed[1, source_core, c].astype(f32)
            )
            first = source_core * half + c * cols
            out_ref[:, first : first + cols] = merged.astype(bf16)

    @pl.when(me == 0)
    def _():
        lax.fori_loop(soon + 1 + CHUNKS, wrapped, cross, 0)

    @pl.when(me < last)
    def _():
        def up_sent(step, carry):
            for kind in range(3):
                up_copy(kind, me, step).wait_send()
            return carry

        lax.fori_loop(0, jnp.minimum(me, hops - 1) + 1, up_sent, 0)
        rim_copy.wait_send()

    def down_sent(slot, carry):
        for kind in range(3):
            down_copy(kind, slot).wait_send()
        return carry

    lax.fori_loop(
        jnp.where(low, me, 0),
        jnp.where(low, wrapped, jnp.maximum(me - hops - 1, 0)),
        down_sent,
        0,
    )
    att_w_copy.wait_send()
    pool_w_copy.wait_send()
    pool_mix_copy.wait_send()
    att_mix_copy.wait_send()
    for c in range(CHUNKS):
        for copy in relay_copies(c):
            copy.wait_send()
        land_copy(0, chip_right, 1, c).wait_send()
        land_copy(1, chip_left, 0, c).wait_send()
        land_copy(0, chip_right, 0, c).wait_send()
        land_copy(1, chip_left, 1, c).wait_send()
        home_copy(c).wait_send()


def body(
    n_sp,
    n_tp,
    query_rows,
    key_rows,
    value_rows,
    pool_input,
    log_gate_sums,
    query_gain,
    key_gain,
    pool_weight,
    pool_scale,
    attention_out,
    pooling_out,
):
    length = query_rows.shape[0]
    heads = query_rows.shape[1] // HEAD
    group = pool_input.shape[1]
    width = attention_out.shape[1]
    half = width // 2
    cols = half // CHUNKS
    rows = length // n_tp
    gate_tile = -(-heads * length // LANES // 8) * 8
    wrapped = min(WRAPPED, (n_sp - 1) // 2)
    hops = n_sp - 1 - wrapped
    vmem = pl.BlockSpec(memory_space=pltpu.VMEM)
    dma = pltpu.SemaphoreType.DMA
    return pl.pallas_call(
        functools.partial(kernel, n_sp, n_tp),
        out_shape=jax.ShapeDtypeStruct((rows, width), bf16),
        in_specs=[vmem] * 9 + [pl.BlockSpec(memory_space=pl.ANY)] * 2,
        out_specs=vmem,
        scratch_shapes=[
            pltpu.VMEM((n_sp, length, HEAD), bf16),
            pltpu.VMEM((n_sp, length, HEAD), bf16),
            pltpu.VMEM((n_sp, gate_tile, LANES), f32),
            pltpu.VMEM((heads, length, HEAD), bf16),
            pltpu.VMEM((heads, length, LANES), f32),
            pltpu.VMEM((heads, length, LANES), f32),
            pltpu.VMEM((heads, length, HEAD), f32),
            pltpu.VMEM((4, length, group), bf16),
            pltpu.VMEM((MAX_WINDOW, group), bf16),
            pltpu.VMEM((2, heads * HEAD, half), bf16),
            pltpu.VMEM((2, group, half), bf16),
            pltpu.VMEM((length, half), f32),
            pltpu.VMEM((n_tp, CHUNKS, rows, cols), bf16),
            pltpu.VMEM((2, CHUNKS, rows, cols), bf16),
            pltpu.VMEM((3, 2, CHUNKS, rows, cols), bf16),
            dma((3, hops)),
            dma((3, hops)),
            dma((3, wrapped)),
            dma((3, wrapped)),
            pltpu.SemaphoreType.REGULAR,
            pltpu.SemaphoreType.REGULAR,
            dma((3,)),
            dma((3,)),
            dma((2,)),
            dma((2,)),
            dma((2,)),
            dma((2, CHUNKS)),
            dma((2, CHUNKS)),
            dma((3, 2, CHUNKS)),
            dma((3, 2, CHUNKS)),
        ],
        compiler_params=pltpu.CompilerParams(
            collective_id=0, has_side_effects=True, vmem_limit_bytes=56 * 1024 * 1024
        ),
    )(
        query_rows,
        key_rows,
        value_rows,
        log_gate_sums.T,
        pool_input,
        query_gain.reshape(1, -1),
        key_gain.reshape(1, -1),
        pool_weight,
        pool_scale.reshape(1, -1),
        attention_out,
        pooling_out,
    )


def solution(mesh):
    return jax.shard_map(
        functools.partial(body, mesh.shape["sp"], mesh.shape["tp"]),
        mesh=mesh,
        in_specs=(
            P(("grp", "sp"), "tp"),
            P(("grp", "sp"), "tp"),
            P(("grp", "sp"), "tp"),
            P(("grp", "sp"), "tp"),
            P(("grp", "sp"), "tp"),
            P(),
            P(),
            P("tp", None, None),
            P("tp"),
            P("tp", None),
            P("tp", None),
        ),
        out_specs=P(("grp", "sp", "tp"), None),
        check_vma=False,
    )
```

```python
import functools
import math

import jax
import jax.numpy as jnp
from jax import lax
from jax.experimental import pallas as pl
from jax.experimental.pallas import tpu as pltpu
from jax.sharding import PartitionSpec as P

HEAD = 128
MAX_WINDOW = 16
LANES = 128
CHUNKS = 4
WRAPPED = 13
LAG = 3
LAST_LAG = 3
UPPER_LAG = 5
SOON_FIRST = 1
SOON = 7
POOL_AFTER = 1
PROJECT_AFTER = 3

epsilon = 1e-06
masked = -1e30
LOG2E = math.log2(math.e)

f32 = jnp.float32
bf16 = jnp.bfloat16


def normed(rows, gain):
    wide = rows.astype(f32)
    scale = lax.rsqrt(jnp.mean(wide * wide, axis=-1, keepdims=True) + epsilon)
    return (wide * scale * gain).astype(bf16)


def rows_dot(a, b):
    return lax.dot_general(a, b, (((1,), (1,)), ((), ())), preferred_element_type=f32)


def dot(a, b):
    return jnp.dot(a, b, preferred_element_type=f32)


def kernel(
    n_sp,
    n_tp,
    q_ref,
    k_ref,
    v_ref,
    gate_ref,
    pool_ref,
    q_gain_ref,
    k_gain_ref,
    pool_w_ref,
    pool_s_ref,
    att_w_hbm,
    pool_w_out_hbm,
    out_ref,
    keys,
    values,
    gates,
    queries,
    best,
    total,
    acc,
    mix,
    rim,
    w_att,
    w_pool,
    pool_part,
    parts,
    relay,
    landed,
    up_send,
    up_recv,
    down_send,
    down_recv,
    ready_sem,
    late_sem,
    early_send,
    early_recv,
    local_sem,
    mix_send,
    mix_recv,
    relay_send,
    relay_recv,
    land_send,
    land_recv,
):
    me = lax.axis_index("sp")
    tp = lax.axis_index("tp")
    length = q_ref.shape[0]
    heads = q_ref.shape[1] // HEAD
    pieces = length // LANES
    n_x = n_tp // 2
    core = lax.rem(tp, 2)
    other = 1 - core
    chip = tp // 2
    chip_right = lax.rem(chip + 1, n_x)
    chip_left = lax.rem(chip + n_x - 1, n_x)
    chip_far = lax.rem(chip + 2, n_x)
    above = lax.rem(me + 1, n_sp)
    below = lax.rem(me + n_sp - 1, n_sp)
    wrapped = min(WRAPPED, (n_sp - 1) // 2)
    hops = n_sp - 1 - wrapped
    last = n_sp - 1
    half = out_ref.shape[1] // 2
    cols = half // CHUNKS
    rows = out_ref.shape[0]

    def remote(src, dst, send_sem, recv_sem, **where):
        return pltpu.make_async_remote_copy(
            src_ref=src,
            dst_ref=dst,
            send_sem=send_sem,
            recv_sem=recv_sem,
            device_id=where,
            device_id_type=pl.DeviceIdType.MESH,
        )

    barrier = pltpu.get_barrier_semaphore()
    first = jnp.logical_and(me == 0, tp == 0)
    beside_z = jnp.logical_and(tp == 0, me == 1)
    beside_chip = jnp.logical_or(chip == 1, chip == n_x - 1)
    beside_x = jnp.logical_and(me == 0, jnp.logical_or(tp == 1, beside_chip))
    beside = jnp.logical_or(beside_z, beside_x)

    def signal(sem, where):
        pl.semaphore_signal(
            sem, inc=1, device_id=where, device_id_type=pl.DeviceIdType.MESH
        )

    neighbours = (
        {"tp": 2 * chip + other},
        {"tp": 2 * chip_right},
        {"tp": 2 * chip_right + 1},
        {"tp": 2 * chip_left},
        {"tp": 2 * chip_left + 1},
    )

    signal(barrier, {"sp": below})

    @pl.when(jnp.logical_not(first))
    def _():
        @pl.when(me < last)
        def _():
            signal(barrier, {"sp": above})

        for where in neighbours:
            signal(barrier, where)

    my_cols = pl.ds(pl.multiple_of(core * half, LANES), half)
    other_cols = pl.ds(pl.multiple_of(other * half, LANES), half)
    load_att = pltpu.make_async_copy(att_w_hbm.at[:, my_cols], w_att.at[0], local_sem.at[0])
    load_pool = pltpu.make_async_copy(
        pool_w_out_hbm.at[:, my_cols], w_pool.at[0], local_sem.at[1]
    )
    load_att.start()
    load_pool.start()

    keys[me] = normed(k_ref[...], k_gain_ref[...])
    values[me] = v_ref[...]
    gates[me] = jnp.concatenate(
        [
            gate_ref[h : h + 1, c * LANES : (c + 1) * LANES]
            for h in range(heads)
            for c in range(pieces)
        ]
        + [jnp.zeros((-(heads * pieces) % 8, LANES), f32)],
        axis=0,
    )
    for h in range(heads):
        queries[h] = normed(q_ref[:, h * HEAD : (h + 1) * HEAD], q_gain_ref[...])

    arrivals = 7 - jnp.where(me == 0, 1, 0) - jnp.where(beside, 1, 0)
    pl.semaphore_wait(barrier, arrivals)

    @pl.when(first)
    def _():
        signal(late_sem, {"sp": above})
        for where in neighbours:
            signal(late_sem, where)

    @pl.when(me == last)
    def _():
        signal(ready_sem, {"sp": above})

    stores = (values, gates, keys)

    def up_copy(kind, slot, step):
        return remote(
            stores[kind].at[slot],
            stores[kind].at[slot],
            up_send.at[kind, step],
            up_recv.at[kind, step],
            sp=above,
        )

    def down_copy(kind, slot):
        return remote(
            stores[kind].at[slot],
            stores[kind].at[slot],
            down_send.at[kind, slot],
            down_recv.at[kind, slot],
            sp=below,
        )

    rim_copy = remote(
        pool_ref.at[pl.ds(length - MAX_WINDOW, MAX_WINDOW)],
        rim,
        early_send.at[0],
        early_recv.at[0],
        sp=above,
    )
    @pl.when(me < last)
    def _():
        rim_copy.start()
        for kind in range(3):
            up_copy(kind, me, 0).start()

    def start_down():
        for kind in range(3):
            down_copy(kind, me).start()

    starts_down = jnp.logical_and(me > 0, me < wrapped)

    @pl.when(jnp.logical_and(starts_down, jnp.logical_not(beside)))
    def _():
        start_down()

    att_w_copy = remote(
        att_w_hbm.at[:, other_cols],
        w_att.at[1],
        early_send.at[1],
        early_recv.at[1],
        tp=2 * chip + other,
    )
    pool_w_copy = remote(
        pool_w_out_hbm.at[:, other_cols],
        w_pool.at[1],
        early_send.at[2],
        early_recv.at[2],
        tp=2 * chip + other,
    )
    scale = LOG2E / math.sqrt(HEAD)

    def score_pieces(h, slot):
        z = rows_dot(queries[h], keys[slot])
        base = gate_ref[h : h + 1, 0:1]
        lifted = (base - gates[slot]) * LOG2E
        return [
            z[:, c * LANES : (c + 1) * LANES] * scale
            + lifted[h * pieces + c : h * pieces + c + 1, :]
            for c in range(pieces)
        ]

    def row_max(score):
        most = functools.reduce(jnp.maximum, score)
        return jnp.max(most, axis=-1, keepdims=True)

    def weigh(score, top):
        weights = [jnp.exp2(s - top) for s in score]
        return functools.reduce(jnp.add, weights), jnp.concatenate(
            [w.astype(bf16) for w in weights], axis=1
        )

    def attend_own():
        for h in range(heads):
            score = score_pieces(h, me)
            position = lax.broadcasted_iota(jnp.int32, (length, LANES), 0)
            lane = lax.broadcasted_iota(jnp.int32, (length, LANES), 1)
            score = [
                jnp.where(lane + c * LANES <= position, s, masked) for c, s in enumerate(score)
            ]
            top = jnp.broadcast_to(row_max(score), (length, LANES))
            summed, weights = weigh(score, top)
            best[h] = top
            total[h] = summed
            acc[h] = dot(weights, values[me])

    def attend(slot):
        for h in range(heads):
            score = score_pieces(h, slot)
            before = best[h]
            top = jnp.maximum(before, row_max(score))
            fade = jnp.exp2(before - top)
            summed, weights = weigh(score, top)
            best[h] = top
            total[h] = total[h] * fade + summed
            acc[h] = acc[h] * fade + dot(weights, values[slot])

    attend_own()

    level_count = MAX_WINDOW.bit_length() - 1
    level = lax.rem(tp, level_count)

    def pooling():
        @pl.when(me == 0)
        def _():
            rim[...] = jnp.zeros_like(rim)

        @pl.when(me > 0)
        def _():
            rim_copy.wait_recv()

        edge = rim[...].astype(f32)
        here = pool_ref[...].astype(f32)
        window_sum = jnp.concatenate([edge, here], axis=0)
        chosen = jnp.zeros_like(here)
        for k in range(level_count):
            window_sum = window_sum + pltpu.roll(window_sum, 1 << k, 0)
            chosen = jnp.where(level == k, window_sum[MAX_WINDOW:], chosen)
        window = (2 << level).astype(f32) if hasattr(level, "astype") else float(2 << level)
        position = me * length + lax.broadcasted_iota(jnp.int32, here.shape, 0)
        counts = jnp.minimum(position.astype(f32) + 1.0, window)
        pooled = (chosen / counts - here).astype(bf16)
        mixed = dot(pooled, pool_w_ref[0]) * pool_s_ref[...]
        mix[0] = mixed.astype(bf16)

    def cross(slot, carry):
        for kind in range(3):
            down_copy(kind, slot).wait_recv()
            down_copy(kind, slot).start()
        return carry

    soon = jnp.where(first, SOON_FIRST, SOON)

    @pl.when(me == 0)
    def _():
        pl.semaphore_wait(ready_sem, 1)
        for kind in range(3):
            down_copy(kind, 0).start()
        lax.fori_loop(1, soon, cross, 0)

    @pl.when(beside)
    def _():
        pl.semaphore_wait(late_sem, 1)

        @pl.when(starts_down)
        def _():
            start_down()

    att_w_copy.start()
    pool_w_copy.start()
    partner = 2 * chip + other
    pool_mix_copy = remote(
        mix.at[0], mix.at[1], mix_send.at[0], mix_recv.at[0], tp=partner
    )

    low = me < wrapped
    down_lag = jnp.where(me == last, LAST_LAG, UPPER_LAG)
    down_base = jnp.where(low, me - LAG, me - n_sp + 1 - down_lag)
    down_first = jnp.where(low, me + 1, 0)
    down_last = jnp.where(low, wrapped - 1, me - hops - 1)
    up_steps = jnp.minimum(me, hops)

    def has_down(step):
        return jnp.logical_and(down_base + step >= down_first, down_base + step <= down_last)

    def ring_step(step, carry):
        slot_up = jnp.maximum(me - step, 0)
        slot_down = jnp.clip(down_base + step, 0, wrapped - 1)
        takes_up = step <= up_steps
        takes_down = has_down(step)

        def pass_on(kind):
            @pl.when(takes_up)
            def _():
                up_copy(kind, slot_up, step - 1).wait_recv()

            @pl.when(jnp.logical_and(takes_up, jnp.logical_and(step < hops, me < last)))
            def _():
                up_copy(kind, slot_up, step).start()

            @pl.when(takes_down)
            def _():
                down_copy(kind, slot_down).wait_recv()

            @pl.when(jnp.logical_and(takes_down, jnp.logical_or(low, slot_down < down_last)))
            def _():
                down_copy(kind, slot_down).start()

        pass_on(0)
        pass_on(1)

        @pl.when(jnp.logical_and(step > 1, step - 1 <= up_steps))
        def _():
            attend(jnp.maximum(me - step + 1, 0))

        pass_on(2)

        @pl.when(jnp.logical_and(me > hops, has_down(step - 1)))
        def _():
            attend(jnp.clip(down_base + step - 1, 0, wrapped - 1))

        return carry

    steps = jnp.where(
        me == 0, 0, jnp.maximum(up_steps + 1, jnp.where(low, wrapped - 1 - me + LAG, 0))
    )
    pool_step = jnp.minimum(steps, POOL_AFTER)
    project_step = jnp.minimum(steps, PROJECT_AFTER)
    lax.fori_loop(1, pool_step + 1, ring_step, 0)
    pooling()
    pool_mix_copy.start()
    lax.fori_loop(pool_step + 1, project_step + 1, ring_step, 0)

    load_att.wait()
    load_pool.wait()
    att_w_copy.wait_recv()
    pool_w_copy.wait_recv()
    pool_mix_copy.wait_recv()
    for c in range(CHUNKS):
        span = pl.ds(c * cols, cols)
        pool_part[:, span] = dot(mix[0], w_pool[0, :, span]) + dot(mix[1], w_pool[1, :, span])

    @pl.when(me == 0)
    def _():
        cross(soon, 0)

    lax.fori_loop(project_step + 1, steps + 1, ring_step, 0)

    for h in range(heads):
        weight_sum = jnp.sum(total[h], axis=-1, keepdims=True)
        mix[2, :, h * HEAD : (h + 1) * HEAD] = (acc[h] / weight_sum).astype(bf16)
    att_mix_copy = remote(mix.at[2], mix.at[3], mix_send.at[1], mix_recv.at[1], tp=partner)
    att_mix_copy.start()
    for c in range(CHUNKS):
        span = pl.ds(c * cols, cols)
        pool_part[:, span] += dot(mix[2], w_att[0, :, span])
    att_mix_copy.wait_recv()

    def relay_copies(c):
        return (
            remote(
                parts.at[2 * chip_far, c],
                relay.at[0, c],
                relay_send.at[0, c],
                relay_recv.at[0, c],
                tp=2 * chip_right + core,
            ),
            remote(
                parts.at[2 * chip_far + 1, c],
                relay.at[1, c],
                relay_send.at[1, c],
                relay_recv.at[1, c],
                tp=2 * chip_left + core,
            ),
        )

    def land_copy(side, target_chip, target_core, c):
        target = 2 * target_chip + target_core
        return remote(
            parts.at[target, c],
            landed.at[side, core, c],
            land_send.at[side, target_core, c],
            land_recv.at[side, core, c],
            tp=target,
        )

    def home_copy(c):
        return remote(
            parts.at[partner, c],
            landed.at[2, core, c],
            land_send.at[2, 0, c],
            land_recv.at[2, core, c],
            tp=partner,
        )

    for c in range(CHUNKS):
        span = pl.ds(c * cols, cols)
        part = (pool_part[:, span] + dot(mix[3], w_att[1, :, span])).astype(bf16)
        for d in range(n_tp):
            parts[d, c] = part[d * rows : (d + 1) * rows]
        for copy in relay_copies(c):
            copy.start()
    for c in range(CHUNKS):
        land_copy(0, chip_right, 1, c).start()
        land_copy(1, chip_left, 0, c).start()

    @pl.when(me == 0)
    def _():
        cross(soon + 1, 0)

    for c in range(CHUNKS):
        home_copy(c).start()
    for c in range(CHUNKS):
        from_left, from_right = relay_copies(c)
        for side, copy, target in (
            (0, from_left, 2 * chip_right),
            (1, from_right, 2 * chip_left + 1),
        ):
            copy.wait_recv()
            joined = parts[target, c].astype(f32) + relay[side, c].astype(f32)
            parts[target, c] = joined.astype(bf16)
        land_copy(0, chip_right, 0, c).start()
        land_copy(1, chip_left, 1, c).start()

        @pl.when(me == 0)
        def _():
            cross(soon + 2 + c, 0)

    def landed_wait(side, source_core, c):
        remote(
            landed.at[side, source_core, c],
            landed.at[side, source_core, c],
            land_send.at[side, 0, c],
            land_recv.at[side, source_core, c],
            tp=partner,
        ).wait_recv()

    for c in range(CHUNKS):
        landed_wait(2, other, c)
        for source_core in range(2):
            landed_wait(0, source_core, c)
            landed_wait(1, source_core, c)
        for source_core in range(2):
            home = jnp.where(
                core == source_core,
                parts[tp, c].astype(f32),
                landed[2, source_core, c].astype(f32),
            )
            merged = (
                home
                + landed[0, source_core, c].astype(f32)
                + landed[1, source_core, c].astype(f32)
            )
            first = source_core * half + c * cols
            out_ref[:, first : first + cols] = merged.astype(bf16)

    @pl.when(me == 0)
    def _():
        lax.fori_loop(soon + 2 + CHUNKS, wrapped, cross, 0)

    @pl.when(me < last)
    def _():
        def up_sent(step, carry):
            for kind in range(3):
                up_copy(kind, me, step).wait_send()
            return carry

        lax.fori_loop(0, jnp.minimum(me, hops - 1) + 1, up_sent, 0)
        rim_copy.wait_send()

    def down_sent(slot, carry):
        for kind in range(3):
            down_copy(kind, slot).wait_send()
        return carry

    lax.fori_loop(
        jnp.where(low, me, 0),
        jnp.where(low, wrapped, jnp.maximum(me - hops - 1, 0)),
        down_sent,
        0,
    )
    att_w_copy.wait_send()
    pool_w_copy.wait_send()
    pool_mix_copy.wait_send()
    att_mix_copy.wait_send()
    for c in range(CHUNKS):
        for copy in relay_copies(c):
            copy.wait_send()
        land_copy(0, chip_right, 1, c).wait_send()
        land_copy(1, chip_left, 0, c).wait_send()
        land_copy(0, chip_right, 0, c).wait_send()
        land_copy(1, chip_left, 1, c).wait_send()
        home_copy(c).wait_send()


def body(
    n_sp,
    n_tp,
    query_rows,
    key_rows,
    value_rows,
    pool_input,
    log_gate_sums,
    query_gain,
    key_gain,
    pool_weight,
    pool_scale,
    attention_out,
    pooling_out,
):
    length = query_rows.shape[0]
    heads = query_rows.shape[1] // HEAD
    group = pool_input.shape[1]
    width = attention_out.shape[1]
    half = width // 2
    cols = half // CHUNKS
    rows = length // n_tp
    gate_tile = -(-heads * length // LANES // 8) * 8
    wrapped = min(WRAPPED, (n_sp - 1) // 2)
    hops = n_sp - 1 - wrapped
    vmem = pl.BlockSpec(memory_space=pltpu.VMEM)
    dma = pltpu.SemaphoreType.DMA
    return pl.pallas_call(
        functools.partial(kernel, n_sp, n_tp),
        out_shape=jax.ShapeDtypeStruct((rows, width), bf16),
        in_specs=[vmem] * 9 + [pl.BlockSpec(memory_space=pl.ANY)] * 2,
        out_specs=vmem,
        scratch_shapes=[
            pltpu.VMEM((n_sp, length, HEAD), bf16),
            pltpu.VMEM((n_sp, length, HEAD), bf16),
            pltpu.VMEM((n_sp, gate_tile, LANES), f32),
            pltpu.VMEM((heads, length, HEAD), bf16),
            pltpu.VMEM((heads, length, LANES), f32),
            pltpu.VMEM((heads, length, LANES), f32),
            pltpu.VMEM((heads, length, HEAD), f32),
            pltpu.VMEM((4, length, group), bf16),
            pltpu.VMEM((MAX_WINDOW, group), bf16),
            pltpu.VMEM((2, heads * HEAD, half), bf16),
            pltpu.VMEM((2, group, half), bf16),
            pltpu.VMEM((length, half), f32),
            pltpu.VMEM((n_tp, CHUNKS, rows, cols), bf16),
            pltpu.VMEM((2, CHUNKS, rows, cols), bf16),
            pltpu.VMEM((3, 2, CHUNKS, rows, cols), bf16),
            dma((3, hops)),
            dma((3, hops)),
            dma((3, wrapped)),
            dma((3, wrapped)),
            pltpu.SemaphoreType.REGULAR,
            pltpu.SemaphoreType.REGULAR,
            dma((3,)),
            dma((3,)),
            dma((2,)),
            dma((2,)),
            dma((2,)),
            dma((2, CHUNKS)),
            dma((2, CHUNKS)),
            dma((3, 2, CHUNKS)),
            dma((3, 2, CHUNKS)),
        ],
        compiler_params=pltpu.CompilerParams(
            collective_id=0, has_side_effects=True, vmem_limit_bytes=56 * 1024 * 1024
        ),
    )(
        query_rows,
        key_rows,
        value_rows,
        log_gate_sums.T,
        pool_input,
        query_gain.reshape(1, -1),
        key_gain.reshape(1, -1),
        pool_weight,
        pool_scale.reshape(1, -1),
        attention_out,
        pooling_out,
    )


def solution(mesh):
    return jax.shard_map(
        functools.partial(body, mesh.shape["sp"], mesh.shape["tp"]),
        mesh=mesh,
        in_specs=(
            P(("grp", "sp"), "tp"),
            P(("grp", "sp"), "tp"),
            P(("grp", "sp"), "tp"),
            P(("grp", "sp"), "tp"),
            P(("grp", "sp"), "tp"),
            P(),
            P(),
            P("tp", None, None),
            P("tp"),
            P("tp", None),
            P("tp", None),
        ),
        out_specs=P(("grp", "sp", "tp"), None),
        check_vma=False,
    )
```

```python
import functools
import math

import jax
import jax.numpy as jnp
from jax import lax
from jax.experimental import pallas as pl
from jax.experimental.pallas import tpu as pltpu
from jax.sharding import PartitionSpec as P

HEAD = 128
MAX_WINDOW = 16
LANES = 128
CHUNKS = 4
WRAPPED = 13
LAG = 3
LAST_LAG = 3
NEAR_LAG = 5
UPPER_LAG = 6
SOON_FIRST = 1
SOON = 4
POOL_AFTER = 1
PROJECT_AFTER = 3

epsilon = 1e-06
masked = -1e30
LOG2E = math.log2(math.e)

f32 = jnp.float32
bf16 = jnp.bfloat16


def normed(rows, gain):
    wide = rows.astype(f32)
    scale = lax.rsqrt(jnp.mean(wide * wide, axis=-1, keepdims=True) + epsilon)
    return (wide * scale * gain).astype(bf16)


def rows_dot(a, b):
    return lax.dot_general(a, b, (((1,), (1,)), ((), ())), preferred_element_type=f32)


def dot(a, b):
    return jnp.dot(a, b, preferred_element_type=f32)


def kernel(
    n_sp,
    n_tp,
    q_ref,
    k_ref,
    v_ref,
    gate_ref,
    pool_ref,
    q_gain_ref,
    k_gain_ref,
    pool_w_ref,
    pool_s_ref,
    att_w_hbm,
    pool_w_out_hbm,
    out_ref,
    keys,
    values,
    gates,
    queries,
    best,
    total,
    acc,
    mix,
    rim,
    w_att,
    w_pool,
    pool_part,
    parts,
    relay,
    landed,
    up_send,
    up_recv,
    down_send,
    down_recv,
    ready_sem,
    late_sem,
    early_send,
    early_recv,
    local_sem,
    mix_send,
    mix_recv,
    relay_send,
    relay_recv,
    land_send,
    land_recv,
):
    me = lax.axis_index("sp")
    tp = lax.axis_index("tp")
    length = q_ref.shape[0]
    heads = q_ref.shape[1] // HEAD
    pieces = length // LANES
    n_x = n_tp // 2
    core = lax.rem(tp, 2)
    other = 1 - core
    chip = tp // 2
    chip_right = lax.rem(chip + 1, n_x)
    chip_left = lax.rem(chip + n_x - 1, n_x)
    chip_far = lax.rem(chip + 2, n_x)
    above = lax.rem(me + 1, n_sp)
    below = lax.rem(me + n_sp - 1, n_sp)
    wrapped = min(WRAPPED, (n_sp - 1) // 2)
    hops = n_sp - 1 - wrapped
    last = n_sp - 1
    half = out_ref.shape[1] // 2
    cols = half // CHUNKS
    rows = out_ref.shape[0]

    def remote(src, dst, send_sem, recv_sem, **where):
        return pltpu.make_async_remote_copy(
            src_ref=src,
            dst_ref=dst,
            send_sem=send_sem,
            recv_sem=recv_sem,
            device_id=where,
            device_id_type=pl.DeviceIdType.MESH,
        )

    barrier = pltpu.get_barrier_semaphore()
    first = jnp.logical_and(me == 0, tp == 0)
    beside_z = jnp.logical_and(tp == 0, me == 1)
    beside_chip = jnp.logical_or(chip == 1, chip == n_x - 1)
    beside_x = jnp.logical_and(me == 0, jnp.logical_or(tp == 1, beside_chip))
    beside = jnp.logical_or(beside_z, beside_x)

    def signal(sem, where):
        pl.semaphore_signal(
            sem, inc=1, device_id=where, device_id_type=pl.DeviceIdType.MESH
        )

    neighbours = (
        {"tp": 2 * chip + other},
        {"tp": 2 * chip_right},
        {"tp": 2 * chip_right + 1},
        {"tp": 2 * chip_left},
        {"tp": 2 * chip_left + 1},
    )

    signal(barrier, {"sp": below})

    @pl.when(jnp.logical_not(first))
    def _():
        @pl.when(me < last)
        def _():
            signal(barrier, {"sp": above})

        for where in neighbours:
            signal(barrier, where)

    my_cols = pl.ds(pl.multiple_of(core * half, LANES), half)
    other_cols = pl.ds(pl.multiple_of(other * half, LANES), half)
    load_att = pltpu.make_async_copy(att_w_hbm.at[:, my_cols], w_att.at[0], local_sem.at[0])
    load_pool = pltpu.make_async_copy(
        pool_w_out_hbm.at[:, my_cols], w_pool.at[0], local_sem.at[1]
    )
    load_att.start()
    load_pool.start()

    keys[me] = normed(k_ref[...], k_gain_ref[...])
    values[me] = v_ref[...]
    gates[me] = jnp.concatenate(
        [
            gate_ref[h : h + 1, c * LANES : (c + 1) * LANES]
            for h in range(heads)
            for c in range(pieces)
        ]
        + [jnp.zeros((-(heads * pieces) % 8, LANES), f32)],
        axis=0,
    )
    for h in range(heads):
        queries[h] = normed(q_ref[:, h * HEAD : (h + 1) * HEAD], q_gain_ref[...])

    arrivals = 7 - jnp.where(me == 0, 1, 0) - jnp.where(beside, 1, 0)
    pl.semaphore_wait(barrier, arrivals)

    @pl.when(first)
    def _():
        signal(late_sem, {"sp": above})
        for where in neighbours:
            signal(late_sem, where)

    @pl.when(me == last)
    def _():
        signal(ready_sem, {"sp": above})

    stores = (values, gates, keys)

    def up_copy(kind, slot, step):
        return remote(
            stores[kind].at[slot],
            stores[kind].at[slot],
            up_send.at[kind, step],
            up_recv.at[kind, step],
            sp=above,
        )

    def down_copy(kind, slot):
        return remote(
            stores[kind].at[slot],
            stores[kind].at[slot],
            down_send.at[kind, slot],
            down_recv.at[kind, slot],
            sp=below,
        )

    rim_copy = remote(
        pool_ref.at[pl.ds(length - MAX_WINDOW, MAX_WINDOW)],
        rim,
        early_send.at[0],
        early_recv.at[0],
        sp=above,
    )
    @pl.when(me < last)
    def _():
        rim_copy.start()
        for kind in range(3):
            up_copy(kind, me, 0).start()

    def start_down():
        for kind in range(3):
            down_copy(kind, me).start()

    starts_down = jnp.logical_and(me > 0, me < wrapped)

    @pl.when(jnp.logical_and(starts_down, jnp.logical_not(beside)))
    def _():
        start_down()

    att_w_copy = remote(
        att_w_hbm.at[:, other_cols],
        w_att.at[1],
        early_send.at[1],
        early_recv.at[1],
        tp=2 * chip + other,
    )
    pool_w_copy = remote(
        pool_w_out_hbm.at[:, other_cols],
        w_pool.at[1],
        early_send.at[2],
        early_recv.at[2],
        tp=2 * chip + other,
    )
    scale = LOG2E / math.sqrt(HEAD)

    def score_pieces(h, slot):
        z = rows_dot(queries[h], keys[slot])
        base = gate_ref[h : h + 1, 0:1]
        lifted = (base - gates[slot]) * LOG2E
        return [
            z[:, c * LANES : (c + 1) * LANES] * scale
            + lifted[h * pieces + c : h * pieces + c + 1, :]
            for c in range(pieces)
        ]

    def row_max(score):
        most = functools.reduce(jnp.maximum, score)
        return jnp.max(most, axis=-1, keepdims=True)

    def weigh(score, top):
        weights = [jnp.exp2(s - top) for s in score]
        return functools.reduce(jnp.add, weights), jnp.concatenate(
            [w.astype(bf16) for w in weights], axis=1
        )

    def attend_own():
        for h in range(heads):
            score = score_pieces(h, me)
            position = lax.broadcasted_iota(jnp.int32, (length, LANES), 0)
            lane = lax.broadcasted_iota(jnp.int32, (length, LANES), 1)
            score = [
                jnp.where(lane + c * LANES <= position, s, masked) for c, s in enumerate(score)
            ]
            top = jnp.broadcast_to(row_max(score), (length, LANES))
            summed, weights = weigh(score, top)
            best[h] = top
            total[h] = summed
            acc[h] = dot(weights, values[me])

    def attend(slot):
        for h in range(heads):
            score = score_pieces(h, slot)
            before = best[h]
            top = jnp.maximum(before, row_max(score))
            fade = jnp.exp2(before - top)
            summed, weights = weigh(score, top)
            best[h] = top
            total[h] = total[h] * fade + summed
            acc[h] = acc[h] * fade + dot(weights, values[slot])

    attend_own()

    level_count = MAX_WINDOW.bit_length() - 1
    level = lax.rem(tp, level_count)

    def pooling():
        @pl.when(me == 0)
        def _():
            rim[...] = jnp.zeros_like(rim)

        @pl.when(me > 0)
        def _():
            rim_copy.wait_recv()

        edge = rim[...].astype(f32)
        here = pool_ref[...].astype(f32)
        window_sum = jnp.concatenate([edge, here], axis=0)
        chosen = jnp.zeros_like(here)
        for k in range(level_count):
            window_sum = window_sum + pltpu.roll(window_sum, 1 << k, 0)
            chosen = jnp.where(level == k, window_sum[MAX_WINDOW:], chosen)
        window = (2 << level).astype(f32) if hasattr(level, "astype") else float(2 << level)
        position = me * length + lax.broadcasted_iota(jnp.int32, here.shape, 0)
        counts = jnp.minimum(position.astype(f32) + 1.0, window)
        pooled = (chosen / counts - here).astype(bf16)
        mixed = dot(pooled, pool_w_ref[0]) * pool_s_ref[...]
        mix[0] = mixed.astype(bf16)

    def cross(slot, carry):
        for kind in range(3):
            down_copy(kind, slot).wait_recv()
            down_copy(kind, slot).start()
        return carry

    soon = jnp.where(first, SOON_FIRST, SOON)

    @pl.when(me == 0)
    def _():
        pl.semaphore_wait(ready_sem, 1)
        for kind in range(3):
            down_copy(kind, 0).start()

    @pl.when(beside)
    def _():
        pl.semaphore_wait(late_sem, 1)

        @pl.when(starts_down)
        def _():
            start_down()

    att_w_copy.start()
    pool_w_copy.start()

    @pl.when(me == 0)
    def _():
        lax.fori_loop(1, soon, cross, 0)

    partner = 2 * chip + other
    pool_mix_copy = remote(
        mix.at[0], mix.at[1], mix_send.at[0], mix_recv.at[0], tp=partner
    )

    low = me < wrapped
    down_lag = jnp.where(
        me == last, LAST_LAG, jnp.where(me >= last - 2, NEAR_LAG, UPPER_LAG)
    )
    down_base = jnp.where(low, me - LAG, me - n_sp + 1 - down_lag)
    down_first = jnp.where(low, me + 1, 0)
    down_last = jnp.where(low, wrapped - 1, me - hops - 1)
    up_steps = jnp.minimum(me, hops)

    def has_down(step):
        return jnp.logical_and(down_base + step >= down_first, down_base + step <= down_last)

    def ring_step(step, carry):
        slot_up = jnp.maximum(me - step, 0)
        slot_down = jnp.clip(down_base + step, 0, wrapped - 1)
        takes_up = step <= up_steps
        takes_down = has_down(step)

        def pass_on(kind):
            @pl.when(takes_up)
            def _():
                up_copy(kind, slot_up, step - 1).wait_recv()

            @pl.when(jnp.logical_and(takes_up, jnp.logical_and(step < hops, me < last)))
            def _():
                up_copy(kind, slot_up, step).start()

            @pl.when(takes_down)
            def _():
                down_copy(kind, slot_down).wait_recv()

            @pl.when(jnp.logical_and(takes_down, jnp.logical_or(low, slot_down < down_last)))
            def _():
                down_copy(kind, slot_down).start()

        pass_on(0)
        pass_on(1)

        @pl.when(jnp.logical_and(step > 1, step - 1 <= up_steps))
        def _():
            attend(jnp.maximum(me - step + 1, 0))

        pass_on(2)

        @pl.when(jnp.logical_and(me > hops, has_down(step - 1)))
        def _():
            attend(jnp.clip(down_base + step - 1, 0, wrapped - 1))

        return carry

    steps = jnp.where(
        me == 0, 0, jnp.maximum(up_steps + 1, jnp.where(low, wrapped - 1 - me + LAG, 0))
    )
    pool_step = jnp.minimum(steps, POOL_AFTER)
    project_step = jnp.where(low, steps, jnp.minimum(steps, PROJECT_AFTER))
    lax.fori_loop(1, pool_step + 1, ring_step, 0)
    pooling()
    pool_mix_copy.start()
    lax.fori_loop(pool_step + 1, project_step + 1, ring_step, 0)

    load_att.wait()
    load_pool.wait()
    att_w_copy.wait_recv()
    pool_w_copy.wait_recv()
    pool_mix_copy.wait_recv()
    for c in range(CHUNKS):
        span = pl.ds(c * cols, cols)
        pool_part[:, span] = dot(mix[0], w_pool[0, :, span]) + dot(mix[1], w_pool[1, :, span])

    @pl.when(me == 0)
    def _():
        cross(soon, 0)

    lax.fori_loop(project_step + 1, steps + 1, ring_step, 0)

    for h in range(heads):
        weight_sum = jnp.sum(total[h], axis=-1, keepdims=True)
        mix[2, :, h * HEAD : (h + 1) * HEAD] = (acc[h] / weight_sum).astype(bf16)
    att_mix_copy = remote(mix.at[2], mix.at[3], mix_send.at[1], mix_recv.at[1], tp=partner)
    att_mix_copy.start()
    for c in range(CHUNKS):
        span = pl.ds(c * cols, cols)
        pool_part[:, span] += dot(mix[2], w_att[0, :, span])
    att_mix_copy.wait_recv()

    def relay_copies(c):
        return (
            remote(
                parts.at[2 * chip_far, c],
                relay.at[0, c],
                relay_send.at[0, c],
                relay_recv.at[0, c],
                tp=2 * chip_right + core,
            ),
            remote(
                parts.at[2 * chip_far + 1, c],
                relay.at[1, c],
                relay_send.at[1, c],
                relay_recv.at[1, c],
                tp=2 * chip_left + core,
            ),
        )

    def land_copy(side, target_chip, target_core, c):
        target = 2 * target_chip + target_core
        return remote(
            parts.at[target, c],
            landed.at[side, core, c],
            land_send.at[side, target_core, c],
            land_recv.at[side, core, c],
            tp=target,
        )

    def home_copy(c):
        return remote(
            parts.at[partner, c],
            landed.at[2, core, c],
            land_send.at[2, 0, c],
            land_recv.at[2, core, c],
            tp=partner,
        )

    for c in range(CHUNKS):
        span = pl.ds(c * cols, cols)
        part = (pool_part[:, span] + dot(mix[3], w_att[1, :, span])).astype(bf16)
        for d in range(n_tp):
            parts[d, c] = part[d * rows : (d + 1) * rows]
        for copy in relay_copies(c):
            copy.start()
    for c in range(CHUNKS):
        land_copy(0, chip_right, 1, c).start()
        land_copy(1, chip_left, 0, c).start()

    @pl.when(me == 0)
    def _():
        cross(soon + 1, 0)

    for c in range(CHUNKS):
        home_copy(c).start()
    for c in range(CHUNKS):
        from_left, from_right = relay_copies(c)
        for side, copy, target in (
            (0, from_left, 2 * chip_right),
            (1, from_right, 2 * chip_left + 1),
        ):
            copy.wait_recv()
            joined = parts[target, c].astype(f32) + relay[side, c].astype(f32)
            parts[target, c] = joined.astype(bf16)
        land_copy(0, chip_right, 0, c).start()
        land_copy(1, chip_left, 1, c).start()

        @pl.when(me == 0)
        def _():
            cross(soon + 2 + c, 0)

    def landed_wait(side, source_core, c):
        remote(
            landed.at[side, source_core, c],
            landed.at[side, source_core, c],
            land_send.at[side, 0, c],
            land_recv.at[side, source_core, c],
            tp=partner,
        ).wait_recv()

    for c in range(CHUNKS):
        landed_wait(2, other, c)
        for source_core in range(2):
            landed_wait(0, source_core, c)
            landed_wait(1, source_core, c)
        for source_core in range(2):
            home = jnp.where(
                core == source_core,
                parts[tp, c].astype(f32),
                landed[2, source_core, c].astype(f32),
            )
            merged = (
                home
                + landed[0, source_core, c].astype(f32)
                + landed[1, source_core, c].astype(f32)
            )
            first = source_core * half + c * cols
            out_ref[:, first : first + cols] = merged.astype(bf16)

    @pl.when(me == 0)
    def _():
        lax.fori_loop(soon + 2 + CHUNKS, wrapped, cross, 0)

    @pl.when(me < last)
    def _():
        def up_sent(step, carry):
            for kind in range(3):
                up_copy(kind, me, step).wait_send()
            return carry

        lax.fori_loop(0, jnp.minimum(me, hops - 1) + 1, up_sent, 0)
        rim_copy.wait_send()

    def down_sent(slot, carry):
        for kind in range(3):
            down_copy(kind, slot).wait_send()
        return carry

    lax.fori_loop(
        jnp.where(low, me, 0),
        jnp.where(low, wrapped, jnp.maximum(me - hops - 1, 0)),
        down_sent,
        0,
    )
    att_w_copy.wait_send()
    pool_w_copy.wait_send()
    pool_mix_copy.wait_send()
    att_mix_copy.wait_send()
    for c in range(CHUNKS):
        for copy in relay_copies(c):
            copy.wait_send()
        land_copy(0, chip_right, 1, c).wait_send()
        land_copy(1, chip_left, 0, c).wait_send()
        land_copy(0, chip_right, 0, c).wait_send()
        land_copy(1, chip_left, 1, c).wait_send()
        home_copy(c).wait_send()


def body(
    n_sp,
    n_tp,
    query_rows,
    key_rows,
    value_rows,
    pool_input,
    log_gate_sums,
    query_gain,
    key_gain,
    pool_weight,
    pool_scale,
    attention_out,
    pooling_out,
):
    length = query_rows.shape[0]
    heads = query_rows.shape[1] // HEAD
    group = pool_input.shape[1]
    width = attention_out.shape[1]
    half = width // 2
    cols = half // CHUNKS
    rows = length // n_tp
    gate_tile = -(-heads * length // LANES // 8) * 8
    wrapped = min(WRAPPED, (n_sp - 1) // 2)
    hops = n_sp - 1 - wrapped
    vmem = pl.BlockSpec(memory_space=pltpu.VMEM)
    dma = pltpu.SemaphoreType.DMA
    return pl.pallas_call(
        functools.partial(kernel, n_sp, n_tp),
        out_shape=jax.ShapeDtypeStruct((rows, width), bf16),
        in_specs=[vmem] * 9 + [pl.BlockSpec(memory_space=pl.ANY)] * 2,
        out_specs=vmem,
        scratch_shapes=[
            pltpu.VMEM((n_sp, length, HEAD), bf16),
            pltpu.VMEM((n_sp, length, HEAD), bf16),
            pltpu.VMEM((n_sp, gate_tile, LANES), f32),
            pltpu.VMEM((heads, length, HEAD), bf16),
            pltpu.VMEM((heads, length, LANES), f32),
            pltpu.VMEM((heads, length, LANES), f32),
            pltpu.VMEM((heads, length, HEAD), f32),
            pltpu.VMEM((4, length, group), bf16),
            pltpu.VMEM((MAX_WINDOW, group), bf16),
            pltpu.VMEM((2, heads * HEAD, half), bf16),
            pltpu.VMEM((2, group, half), bf16),
            pltpu.VMEM((length, half), f32),
            pltpu.VMEM((n_tp, CHUNKS, rows, cols), bf16),
            pltpu.VMEM((2, CHUNKS, rows, cols), bf16),
            pltpu.VMEM((3, 2, CHUNKS, rows, cols), bf16),
            dma((3, hops)),
            dma((3, hops)),
            dma((3, wrapped)),
            dma((3, wrapped)),
            pltpu.SemaphoreType.REGULAR,
            pltpu.SemaphoreType.REGULAR,
            dma((3,)),
            dma((3,)),
            dma((2,)),
            dma((2,)),
            dma((2,)),
            dma((2, CHUNKS)),
            dma((2, CHUNKS)),
            dma((3, 2, CHUNKS)),
            dma((3, 2, CHUNKS)),
        ],
        compiler_params=pltpu.CompilerParams(
            collective_id=0, has_side_effects=True, vmem_limit_bytes=56 * 1024 * 1024
        ),
    )(
        query_rows,
        key_rows,
        value_rows,
        log_gate_sums.T,
        pool_input,
        query_gain.reshape(1, -1),
        key_gain.reshape(1, -1),
        pool_weight,
        pool_scale.reshape(1, -1),
        attention_out,
        pooling_out,
    )


def solution(mesh):
    return jax.shard_map(
        functools.partial(body, mesh.shape["sp"], mesh.shape["tp"]),
        mesh=mesh,
        in_specs=(
            P(("grp", "sp"), "tp"),
            P(("grp", "sp"), "tp"),
            P(("grp", "sp"), "tp"),
            P(("grp", "sp"), "tp"),
            P(("grp", "sp"), "tp"),
            P(),
            P(),
            P("tp", None, None),
            P("tp"),
            P("tp", None),
            P("tp", None),
        ),
        out_specs=P(("grp", "sp", "tp"), None),
        check_vma=False,
    )
```

```python
import functools
import math

import jax
import jax.numpy as jnp
from jax import lax
from jax.experimental import pallas as pl
from jax.experimental.pallas import tpu as pltpu
from jax.sharding import PartitionSpec as P

HEAD = 128
MAX_WINDOW = 16
LANES = 128
CHUNKS = 4
WRAPPED = 13
LAG = 2
LAST_LAG = 3
UPPER_LAG = 4
DRIFT = 6
SOON_FIRST = 1
SOON = 4
POOL_AFTER = 1
PROJECT_AFTER = 3

epsilon = 1e-06
masked = -1e30
LOG2E = math.log2(math.e)

f32 = jnp.float32
bf16 = jnp.bfloat16


def normed(rows, gain):
    wide = rows.astype(f32)
    scale = lax.rsqrt(jnp.mean(wide * wide, axis=-1, keepdims=True) + epsilon)
    return (wide * scale * gain).astype(bf16)


def rows_dot(a, b):
    return lax.dot_general(a, b, (((1,), (1,)), ((), ())), preferred_element_type=f32)


def dot(a, b):
    return jnp.dot(a, b, preferred_element_type=f32)


def kernel(
    n_sp,
    n_tp,
    q_ref,
    k_ref,
    v_ref,
    gate_ref,
    pool_ref,
    q_gain_ref,
    k_gain_ref,
    pool_w_ref,
    pool_s_ref,
    att_w_hbm,
    pool_w_out_hbm,
    out_ref,
    keys,
    values,
    gates,
    queries,
    best,
    total,
    acc,
    mix,
    rim,
    w_att,
    w_pool,
    pool_part,
    parts,
    relay,
    landed,
    up_send,
    up_recv,
    down_send,
    down_recv,
    ready_sem,
    late_sem,
    early_send,
    early_recv,
    local_sem,
    mix_send,
    mix_recv,
    relay_send,
    relay_recv,
    land_send,
    land_recv,
):
    me = lax.axis_index("sp")
    tp = lax.axis_index("tp")
    length = q_ref.shape[0]
    heads = q_ref.shape[1] // HEAD
    pieces = length // LANES
    n_x = n_tp // 2
    core = lax.rem(tp, 2)
    other = 1 - core
    chip = tp // 2
    chip_right = lax.rem(chip + 1, n_x)
    chip_left = lax.rem(chip + n_x - 1, n_x)
    chip_far = lax.rem(chip + 2, n_x)
    above = lax.rem(me + 1, n_sp)
    below = lax.rem(me + n_sp - 1, n_sp)
    wrapped = min(WRAPPED, (n_sp - 1) // 2)
    hops = n_sp - 1 - wrapped
    last = n_sp - 1
    half = out_ref.shape[1] // 2
    cols = half // CHUNKS
    rows = out_ref.shape[0]

    def remote(src, dst, send_sem, recv_sem, **where):
        return pltpu.make_async_remote_copy(
            src_ref=src,
            dst_ref=dst,
            send_sem=send_sem,
            recv_sem=recv_sem,
            device_id=where,
            device_id_type=pl.DeviceIdType.MESH,
        )

    barrier = pltpu.get_barrier_semaphore()
    first = jnp.logical_and(me == 0, tp == 0)
    beside_z = jnp.logical_and(tp == 0, me == 1)
    beside_chip = jnp.logical_or(chip == 1, chip == n_x - 1)
    beside_x = jnp.logical_and(me == 0, jnp.logical_or(tp == 1, beside_chip))
    beside = jnp.logical_or(beside_z, beside_x)

    def signal(sem, where):
        pl.semaphore_signal(
            sem, inc=1, device_id=where, device_id_type=pl.DeviceIdType.MESH
        )

    neighbours = (
        {"tp": 2 * chip + other},
        {"tp": 2 * chip_right},
        {"tp": 2 * chip_right + 1},
        {"tp": 2 * chip_left},
        {"tp": 2 * chip_left + 1},
    )

    signal(barrier, {"sp": below})

    @pl.when(jnp.logical_not(first))
    def _():
        @pl.when(me < last)
        def _():
            signal(barrier, {"sp": above})

        for where in neighbours:
            signal(barrier, where)

    my_cols = pl.ds(pl.multiple_of(core * half, LANES), half)
    other_cols = pl.ds(pl.multiple_of(other * half, LANES), half)
    load_att = pltpu.make_async_copy(att_w_hbm.at[:, my_cols], w_att.at[0], local_sem.at[0])
    load_pool = pltpu.make_async_copy(
        pool_w_out_hbm.at[:, my_cols], w_pool.at[0], local_sem.at[1]
    )
    load_att.start()
    load_pool.start()

    keys[me] = normed(k_ref[...], k_gain_ref[...])
    values[me] = v_ref[...]
    gates[me] = jnp.concatenate(
        [
            gate_ref[h : h + 1, c * LANES : (c + 1) * LANES]
            for h in range(heads)
            for c in range(pieces)
        ]
        + [jnp.zeros((-(heads * pieces) % 8, LANES), f32)],
        axis=0,
    )
    for h in range(heads):
        queries[h] = normed(q_ref[:, h * HEAD : (h + 1) * HEAD], q_gain_ref[...])

    arrivals = 7 - jnp.where(me == 0, 1, 0) - jnp.where(beside, 1, 0)
    pl.semaphore_wait(barrier, arrivals)

    @pl.when(first)
    def _():
        signal(late_sem, {"sp": above})
        for where in neighbours:
            signal(late_sem, where)

    @pl.when(me == last)
    def _():
        signal(ready_sem, {"sp": above})

    stores = (values, gates, keys)

    def up_copy(kind, slot, step):
        return remote(
            stores[kind].at[slot],
            stores[kind].at[slot],
            up_send.at[kind, step],
            up_recv.at[kind, step],
            sp=above,
        )

    def down_copy(kind, slot):
        return remote(
            stores[kind].at[slot],
            stores[kind].at[slot],
            down_send.at[kind, slot],
            down_recv.at[kind, slot],
            sp=below,
        )

    rim_copy = remote(
        pool_ref.at[pl.ds(length - MAX_WINDOW, MAX_WINDOW)],
        rim,
        early_send.at[0],
        early_recv.at[0],
        sp=above,
    )
    @pl.when(me < last)
    def _():
        rim_copy.start()
        for kind in range(3):
            up_copy(kind, me, 0).start()

    def start_down():
        for kind in range(3):
            down_copy(kind, me).start()

    starts_down = jnp.logical_and(me > 0, me < wrapped)

    @pl.when(jnp.logical_and(starts_down, jnp.logical_not(beside)))
    def _():
        start_down()

    att_w_copy = remote(
        att_w_hbm.at[:, other_cols],
        w_att.at[1],
        early_send.at[1],
        early_recv.at[1],
        tp=2 * chip + other,
    )
    pool_w_copy = remote(
        pool_w_out_hbm.at[:, other_cols],
        w_pool.at[1],
        early_send.at[2],
        early_recv.at[2],
        tp=2 * chip + other,
    )
    scale = LOG2E / math.sqrt(HEAD)

    def score_pieces(h, slot):
        z = rows_dot(queries[h], keys[slot])
        base = gate_ref[h : h + 1, 0:1]
        lifted = (base - gates[slot]) * LOG2E
        return [
            z[:, c * LANES : (c + 1) * LANES] * scale
            + lifted[h * pieces + c : h * pieces + c + 1, :]
            for c in range(pieces)
        ]

    def row_max(score):
        most = functools.reduce(jnp.maximum, score)
        return jnp.max(most, axis=-1, keepdims=True)

    def weigh(score, top):
        weights = [jnp.exp2(s - top) for s in score]
        return functools.reduce(jnp.add, weights), jnp.concatenate(
            [w.astype(bf16) for w in weights], axis=1
        )

    def attend_own():
        for h in range(heads):
            score = score_pieces(h, me)
            position = lax.broadcasted_iota(jnp.int32, (length, LANES), 0)
            lane = lax.broadcasted_iota(jnp.int32, (length, LANES), 1)
            score = [
                jnp.where(lane + c * LANES <= position, s, masked) for c, s in enumerate(score)
            ]
            top = jnp.broadcast_to(row_max(score), (length, LANES))
            summed, weights = weigh(score, top)
            best[h] = top
            total[h] = summed
            acc[h] = dot(weights, values[me])

    def attend(slot):
        for h in range(heads):
            score = score_pieces(h, slot)
            before = best[h]
            top = jnp.maximum(before, row_max(score))
            fade = jnp.exp2(before - top)
            summed, weights = weigh(score, top)
            best[h] = top
            total[h] = total[h] * fade + summed
            acc[h] = acc[h] * fade + dot(weights, values[slot])

    attend_own()

    level_count = MAX_WINDOW.bit_length() - 1
    level = lax.rem(tp, level_count)

    def pooling():
        @pl.when(me == 0)
        def _():
            rim[...] = jnp.zeros_like(rim)

        @pl.when(me > 0)
        def _():
            rim_copy.wait_recv()

        edge = rim[...].astype(f32)
        here = pool_ref[...].astype(f32)
        window_sum = jnp.concatenate([edge, here], axis=0)
        chosen = jnp.zeros_like(here)
        for k in range(level_count):
            window_sum = window_sum + pltpu.roll(window_sum, 1 << k, 0)
            chosen = jnp.where(level == k, window_sum[MAX_WINDOW:], chosen)
        window = (2 << level).astype(f32) if hasattr(level, "astype") else float(2 << level)
        position = me * length + lax.broadcasted_iota(jnp.int32, here.shape, 0)
        counts = jnp.minimum(position.astype(f32) + 1.0, window)
        pooled = (chosen / counts - here).astype(bf16)
        mixed = dot(pooled, pool_w_ref[0]) * pool_s_ref[...]
        mix[0] = mixed.astype(bf16)

    def cross(slot, carry):
        for kind in range(3):
            down_copy(kind, slot).wait_recv()
            down_copy(kind, slot).start()
        return carry

    soon = jnp.where(first, SOON_FIRST, SOON)

    @pl.when(me == 0)
    def _():
        pl.semaphore_wait(ready_sem, 1)
        for kind in range(3):
            down_copy(kind, 0).start()

    @pl.when(beside)
    def _():
        pl.semaphore_wait(late_sem, 1)

        @pl.when(starts_down)
        def _():
            start_down()

    att_w_copy.start()
    pool_w_copy.start()

    @pl.when(me == 0)
    def _():
        lax.fori_loop(1, soon, cross, 0)

    partner = 2 * chip + other
    pool_mix_copy = remote(
        mix.at[0], mix.at[1], mix_send.at[0], mix_recv.at[0], tp=partner
    )

    low = me < wrapped
    down_lag = jnp.where(
        me == last, LAST_LAG, UPPER_LAG + lax.div(last - me, DRIFT)
    )
    down_base = jnp.where(low, me - LAG, me - n_sp + 1 - down_lag)
    down_first = jnp.where(low, me + 1, 0)
    down_last = jnp.where(low, wrapped - 1, me - hops - 1)
    up_steps = jnp.minimum(me, hops)

    def has_down(step):
        return jnp.logical_and(down_base + step >= down_first, down_base + step <= down_last)

    def ring_step(step, carry):
        slot_up = jnp.maximum(me - step, 0)
        slot_down = jnp.clip(down_base + step, 0, wrapped - 1)
        takes_up = step <= up_steps
        takes_down = has_down(step)

        def pass_on(kind):
            @pl.when(takes_up)
            def _():
                up_copy(kind, slot_up, step - 1).wait_recv()

            @pl.when(jnp.logical_and(takes_up, jnp.logical_and(step < hops, me < last)))
            def _():
                up_copy(kind, slot_up, step).start()

            @pl.when(takes_down)
            def _():
                down_copy(kind, slot_down).wait_recv()

            @pl.when(jnp.logical_and(takes_down, jnp.logical_or(low, slot_down < down_last)))
            def _():
                down_copy(kind, slot_down).start()

        pass_on(0)
        pass_on(1)

        @pl.when(jnp.logical_and(step > 1, step - 1 <= up_steps))
        def _():
            attend(jnp.maximum(me - step + 1, 0))

        pass_on(2)

        @pl.when(jnp.logical_and(me > hops, has_down(step - 1)))
        def _():
            attend(jnp.clip(down_base + step - 1, 0, wrapped - 1))

        return carry

    steps = jnp.where(
        me == 0, 0, jnp.maximum(up_steps + 1, jnp.where(low, wrapped - 1 - me + LAG, 0))
    )
    pool_step = jnp.minimum(steps, POOL_AFTER)
    project_step = jnp.where(low, steps, jnp.minimum(steps, PROJECT_AFTER))
    lax.fori_loop(1, pool_step + 1, ring_step, 0)
    pooling()
    pool_mix_copy.start()
    lax.fori_loop(pool_step + 1, project_step + 1, ring_step, 0)

    load_att.wait()
    load_pool.wait()
    att_w_copy.wait_recv()
    pool_w_copy.wait_recv()
    pool_mix_copy.wait_recv()
    for c in range(CHUNKS):
        span = pl.ds(c * cols, cols)
        pool_part[:, span] = dot(mix[0], w_pool[0, :, span]) + dot(mix[1], w_pool[1, :, span])

    @pl.when(me == 0)
    def _():
        cross(soon, 0)

    lax.fori_loop(project_step + 1, steps + 1, ring_step, 0)

    for h in range(heads):
        weight_sum = jnp.sum(total[h], axis=-1, keepdims=True)
        mix[2, :, h * HEAD : (h + 1) * HEAD] = (acc[h] / weight_sum).astype(bf16)
    att_mix_copy = remote(mix.at[2], mix.at[3], mix_send.at[1], mix_recv.at[1], tp=partner)
    att_mix_copy.start()
    for c in range(CHUNKS):
        span = pl.ds(c * cols, cols)
        pool_part[:, span] += dot(mix[2], w_att[0, :, span])
    att_mix_copy.wait_recv()

    def relay_copies(c):
        return (
            remote(
                parts.at[2 * chip_far, c],
                relay.at[0, c],
                relay_send.at[0, c],
                relay_recv.at[0, c],
                tp=2 * chip_right + core,
            ),
            remote(
                parts.at[2 * chip_far + 1, c],
                relay.at[1, c],
                relay_send.at[1, c],
                relay_recv.at[1, c],
                tp=2 * chip_left + core,
            ),
        )

    def land_copy(side, target_chip, target_core, c):
        target = 2 * target_chip + target_core
        return remote(
            parts.at[target, c],
            landed.at[side, core, c],
            land_send.at[side, target_core, c],
            land_recv.at[side, core, c],
            tp=target,
        )

    def home_copy(c):
        return remote(
            parts.at[partner, c],
            landed.at[2, core, c],
            land_send.at[2, 0, c],
            land_recv.at[2, core, c],
            tp=partner,
        )

    for c in range(CHUNKS):
        span = pl.ds(c * cols, cols)
        part = (pool_part[:, span] + dot(mix[3], w_att[1, :, span])).astype(bf16)
        for d in range(n_tp):
            parts[d, c] = part[d * rows : (d + 1) * rows]
        for copy in relay_copies(c):
            copy.start()
    for c in range(CHUNKS):
        land_copy(0, chip_right, 1, c).start()
        land_copy(1, chip_left, 0, c).start()

    @pl.when(me == 0)
    def _():
        cross(soon + 1, 0)

    for c in range(CHUNKS):
        home_copy(c).start()
    for c in range(CHUNKS):
        from_left, from_right = relay_copies(c)
        for side, copy, target in (
            (0, from_left, 2 * chip_right),
            (1, from_right, 2 * chip_left + 1),
        ):
            copy.wait_recv()
            joined = parts[target, c].astype(f32) + relay[side, c].astype(f32)
            parts[target, c] = joined.astype(bf16)
        land_copy(0, chip_right, 0, c).start()
        land_copy(1, chip_left, 1, c).start()

        @pl.when(me == 0)
        def _():
            cross(soon + 2 + c, 0)

    def landed_wait(side, source_core, c):
        remote(
            landed.at[side, source_core, c],
            landed.at[side, source_core, c],
            land_send.at[side, 0, c],
            land_recv.at[side, source_core, c],
            tp=partner,
        ).wait_recv()

    for c in range(CHUNKS):
        landed_wait(2, other, c)
        for source_core in range(2):
            landed_wait(0, source_core, c)
            landed_wait(1, source_core, c)
        for source_core in range(2):
            home = jnp.where(
                core == source_core,
                parts[tp, c].astype(f32),
                landed[2, source_core, c].astype(f32),
            )
            merged = (
                home
                + landed[0, source_core, c].astype(f32)
                + landed[1, source_core, c].astype(f32)
            )
            first = source_core * half + c * cols
            out_ref[:, first : first + cols] = merged.astype(bf16)

    @pl.when(me == 0)
    def _():
        lax.fori_loop(soon + 2 + CHUNKS, wrapped, cross, 0)

    @pl.when(me < last)
    def _():
        def up_sent(step, carry):
            for kind in range(3):
                up_copy(kind, me, step).wait_send()
            return carry

        lax.fori_loop(0, jnp.minimum(me, hops - 1) + 1, up_sent, 0)
        rim_copy.wait_send()

    def down_sent(slot, carry):
        for kind in range(3):
            down_copy(kind, slot).wait_send()
        return carry

    lax.fori_loop(
        jnp.where(low, me, 0),
        jnp.where(low, wrapped, jnp.maximum(me - hops - 1, 0)),
        down_sent,
        0,
    )
    att_w_copy.wait_send()
    pool_w_copy.wait_send()
    pool_mix_copy.wait_send()
    att_mix_copy.wait_send()
    for c in range(CHUNKS):
        for copy in relay_copies(c):
            copy.wait_send()
        land_copy(0, chip_right, 1, c).wait_send()
        land_copy(1, chip_left, 0, c).wait_send()
        land_copy(0, chip_right, 0, c).wait_send()
        land_copy(1, chip_left, 1, c).wait_send()
        home_copy(c).wait_send()


def body(
    n_sp,
    n_tp,
    query_rows,
    key_rows,
    value_rows,
    pool_input,
    log_gate_sums,
    query_gain,
    key_gain,
    pool_weight,
    pool_scale,
    attention_out,
    pooling_out,
):
    length = query_rows.shape[0]
    heads = query_rows.shape[1] // HEAD
    group = pool_input.shape[1]
    width = attention_out.shape[1]
    half = width // 2
    cols = half // CHUNKS
    rows = length // n_tp
    gate_tile = -(-heads * length // LANES // 8) * 8
    wrapped = min(WRAPPED, (n_sp - 1) // 2)
    hops = n_sp - 1 - wrapped
    vmem = pl.BlockSpec(memory_space=pltpu.VMEM)
    dma = pltpu.SemaphoreType.DMA
    return pl.pallas_call(
        functools.partial(kernel, n_sp, n_tp),
        out_shape=jax.ShapeDtypeStruct((rows, width), bf16),
        in_specs=[vmem] * 9 + [pl.BlockSpec(memory_space=pl.ANY)] * 2,
        out_specs=vmem,
        scratch_shapes=[
            pltpu.VMEM((n_sp, length, HEAD), bf16),
            pltpu.VMEM((n_sp, length, HEAD), bf16),
            pltpu.VMEM((n_sp, gate_tile, LANES), f32),
            pltpu.VMEM((heads, length, HEAD), bf16),
            pltpu.VMEM((heads, length, LANES), f32),
            pltpu.VMEM((heads, length, LANES), f32),
            pltpu.VMEM((heads, length, HEAD), f32),
            pltpu.VMEM((4, length, group), bf16),
            pltpu.VMEM((MAX_WINDOW, group), bf16),
            pltpu.VMEM((2, heads * HEAD, half), bf16),
            pltpu.VMEM((2, group, half), bf16),
            pltpu.VMEM((length, half), f32),
            pltpu.VMEM((n_tp, CHUNKS, rows, cols), bf16),
            pltpu.VMEM((2, CHUNKS, rows, cols), bf16),
            pltpu.VMEM((3, 2, CHUNKS, rows, cols), bf16),
            dma((3, hops)),
            dma((3, hops)),
            dma((3, wrapped)),
            dma((3, wrapped)),
            pltpu.SemaphoreType.REGULAR,
            pltpu.SemaphoreType.REGULAR,
            dma((3,)),
            dma((3,)),
            dma((2,)),
            dma((2,)),
            dma((2,)),
            dma((2, CHUNKS)),
            dma((2, CHUNKS)),
            dma((3, 2, CHUNKS)),
            dma((3, 2, CHUNKS)),
        ],
        compiler_params=pltpu.CompilerParams(
            collective_id=0, has_side_effects=True, vmem_limit_bytes=56 * 1024 * 1024
        ),
    )(
        query_rows,
        key_rows,
        value_rows,
        log_gate_sums.T,
        pool_input,
        query_gain.reshape(1, -1),
        key_gain.reshape(1, -1),
        pool_weight,
        pool_scale.reshape(1, -1),
        attention_out,
        pooling_out,
    )


def solution(mesh):
    return jax.shard_map(
        functools.partial(body, mesh.shape["sp"], mesh.shape["tp"]),
        mesh=mesh,
        in_specs=(
            P(("grp", "sp"), "tp"),
            P(("grp", "sp"), "tp"),
            P(("grp", "sp"), "tp"),
            P(("grp", "sp"), "tp"),
            P(("grp", "sp"), "tp"),
            P(),
            P(),
            P("tp", None, None),
            P("tp"),
            P("tp", None),
            P("tp", None),
        ),
        out_specs=P(("grp", "sp", "tp"), None),
        check_vma=False,
    )
```
